256 devices in a mesh: sp: 64 (over z, x, core), tp: 4 (over y).
Axes of the slice: x: 4, y: 4, z: 8, core: 2. Of those that a mesh axis runs over, the one named last changes fastest.
Arguments:
- conv_out: bfloat16 [12288, 2048], P('sp', 'tp'), may hold values from -6 to 6
- gate_in: bfloat16 [12288, 2048], P('sp', 'tp'), may hold values from -6 to 6
- block_states: float32 [64, 2048], P('sp', 'tp'), may hold values from -4 to 4
- decay_param: float32 [2048], P('tp'), may hold values from 4 to 20
- decay_shift: float32 [12288], P('sp'), may hold values from -2 to 0, as said below
- w_reset: bfloat16 [16, 128, 128], P('tp'), may hold values from -0.5 to 0.5
- w_input: bfloat16 [16, 128, 128], P('tp'), may hold values from -0.5 to 0.5
- w_out: bfloat16 [2048, 2048], P('tp'), may hold values from -0.125 to 0.125
- mixed: bfloat16 [12288, 2048], P('sp', 'tp'), may hold values from -6 to 6
- d_out: bfloat16 [12288, 2048], P('sp', 'tp'), may hold values from -16 to 16
- expert_ids: int32 [12288, 2], P('sp'), may hold values from 0 to 63, all different within a row; in each aligned block of 192 rows (0 to 191, 192 to 383, ...) at most 12 rows name the same one
- route_weights: float32 [12288, 2], P('sp'), may hold values from 0.2 to 1.4
- w_gate: bfloat16 [64, 2048, 1024], P('sp', None, 'tp'), may hold values from -0.125 to 0.125
- w_up: bfloat16 [64, 2048, 1024], P('sp', None, 'tp'), may hold values from -0.125 to 0.125
- w_down: bfloat16 [64, 1024, 2048], P('sp', 'tp'), may hold values from -0.1875 to 0.1875
Outputs:
- grad_w_gate: float32 [64, 2048, 1024], P('sp', None, 'tp')
- grad_w_up: float32 [64, 2048, 1024], P('sp', None, 'tp')
- grad_w_down: float32 [64, 1024, 2048], P('sp', 'tp')
- grad_out_proj_t: float32 [2048, 2048], P('sp', 'tp')
- recurrence_input_gradient: bfloat16 [12288, 2048], P('sp', 'tp')
- grad_gate: bfloat16 [12288, 2048], P('sp', 'tp')
The draws below stay inside these ranges and needn't reach their ends.
Inputs may be any that keep to these rules, and one draw needn't show every extreme that they name: `expert_ids`: each row names 2 different experts; among the 192 tokens of one index of sp no expert is named more than 12 times, and in some index of sp one expert is named exactly 12 times. decay_shift is at most -0.05 / 12288 at every position.
All inputs are finite; a program needn't handle non-finite values.
Results may differ from the reference program's by a relative error of at most 0.013.
Values may be sent and summed in bfloat16 or wider, within the bound.
No kernel may reach another device: no remote copies, remote signals or barrier semaphores. Data moves between devices by JAX's collectives and lax.ppermute only.
A program may use at most 128 MiB of HBM per device.

```python
import math
import jax
import jax.numpy as jnp
import numpy as np
from jax import lax

D = 2048
HEADS = 16
HEAD_DIM = 128
DR = 2048
FE = 1024
TOP = 2
TOK_DEV = 192
SEQUENCE_TOKENS = 12288
EXPERTS = 64
CAP = 12
N_SP = 64
N_TP = 4


def draw_decay_param(key, part):
    chooser, slow_key, fast_key = jax.random.split(jax.random.fold_in(key, 11), 3)
    portion = 0.5
    is_slow = jax.random.uniform(chooser, (DR,), jnp.float32) < portion
    slow_rate = jax.random.uniform(slow_key, (DR,), jnp.float32, minval=0.1, maxval=0.4) / (4.0 * SEQUENCE_TOKENS)
    fast_rate = 1.0 / (4.0 * jax.random.uniform(fast_key, (DR,), jnp.float32, minval=30.0, maxval=100.0))
    rates = jnp.where(is_slow, slow_rate, fast_rate)
    return (-jnp.log(jnp.expm1(rates))).astype(jnp.float32)


def draw_decay_shift(key, part):
    level_key, location_key, depth_key = jax.random.split(jax.random.fold_in(key, 23), 3)
    blocks = SEQUENCE_TOKENS // TOK_DEV
    levels = jnp.exp(jax.random.uniform(level_key, (blocks,), jnp.float32, minval=math.log(0.05), maxval=math.log(0.4)))
    reference_value = -jnp.repeat(levels, TOK_DEV) / SEQUENCE_TOKENS
    spike_locations = jax.random.randint(location_key, (2,), 0, SEQUENCE_TOKENS)
    nesting_levels = jax.random.uniform(depth_key, (2,), jnp.float32, minval=math.log(0.6), maxval=math.log(0.8))
    return reference_value.at[spike_locations].add(nesting_levels).astype(jnp.float32)


def raised(entries, key, source, target, blocks, factor):
    owner, partner = [(jnp.arange(entries.shape[position]) // (entries.shape[position] // blocks)).reshape([-1 if axis == position else 1 for axis in range(entries.ndim)]) for position in (source, target)]
    chosen = jax.random.permutation(key, blocks)[partner]
    strong = (owner == chosen) | (owner == (partner + blocks // 2) % blocks)
    return jnp.where(strong, factor * entries, entries)


def shard_levels(key, extent, cuts, smallest, high):
    def one(axis_at, parts):
        draws = jax.random.uniform(jax.random.fold_in(jax.random.fold_in(key, 6), axis_at), (parts,), jnp.float32, smallest / len(cuts), high / len(cuts))
        return jnp.repeat(jnp.exp(draws), extent[axis_at] // parts).reshape((-1,) + (1,) * (len(extent) - axis_at - 1))

    gain = one(*cuts[0])
    for cut in cuts[1:]:
        gain = gain * one(*cut)
    return gain


def assign_block(own_key, own, number, rows, count, top, limit, lean):
    ranking = jax.random.permutation(own_key, count)
    packed, ordinary = portions_of(count, rows * top, limit, lean, True), portions_of(count, rows * top, limit, lean, False)
    places = jnp.arange(count)

    def named(lengths, offset_by):
        used = int((lengths > 0).sum())
        fixed = max(1, used // 4)
        passed = fixed + (places - fixed + offset_by * (used - fixed)) % max(1, count - fixed)
        return jnp.zeros((count,), jnp.int32).at[ranking[jnp.where(places < fixed, places, passed)]].set(jnp.asarray(lengths, jnp.int32))

    lengths = jnp.where(number % 4 == 0, named(packed, number // 4), named(ordinary, number - number // 4 - 1))
    mixed = jax.random.permutation(jax.random.fold_in(own, 3), count)
    giver, sink = mixed[0:count // 2 * 2:2], mixed[1:count // 2 * 2:2]
    margin = jnp.minimum(lengths[giver] - 1, limit - lengths[sink]) // 2
    margin = jnp.where((giver == ranking[0]) | (sink == ranking[0]) | (lengths[sink] == 0), 0, jnp.maximum(margin, 0))
    passed = jax.random.randint(jax.random.fold_in(own, 4), (count // 2,), 0, 1 << 20) % (margin + 1)
    lengths = lengths.at[giver].add(-passed).at[sink].add(passed)
    items = jnp.searchsorted(jnp.cumsum(lengths), jnp.arange(rows * top), side="right").astype(jnp.int32)
    listing = items.reshape(top, rows).T
    listing = listing[jax.random.permutation(jax.random.fold_in(own, 1), rows)]
    offset_by = jax.random.randint(jax.random.fold_in(own, 2), (rows, 1), 0, top)
    return jnp.take_along_axis(listing, (jnp.arange(top)[None, :] + offset_by) % top, axis=1)


def portions_of(count, total, limit, lean, full):
    weights = [(1 << 20) // math.isqrt(grade ** lean) + 1 for grade in range(1, count + 1)]
    largest = limit if full else min(limit, max(-(-total // count), total * weights[0] // sum(weights)))
    least = 1 if total - largest >= count - 1 else 0
    given, rest = [largest] + [least] * (count - 1), total - largest - least * (count - 1)
    while rest > 0:
        candidates = [i for i in range(1, count) if given[i] < largest] or [i for i in range(1, count) if given[i] < limit]
        whole, left = sum([weights[i] for i in candidates]), rest
        for i in candidates:
            more = min(limit - given[i], max(1, left * weights[i] // whole), rest)
            given[i] = given[i] + more
            rest = rest - more
    return np.array(given)


def bell_draw(own_key, shape, width, bound, cuts=(), kind=jnp.bfloat16):
    drawn = jax.random.normal(own_key, shape, jnp.float32) * width
    if len(cuts) > 0:
        drawn = shard_levels(own_key, shape, cuts, -0.22, 0.18) * drawn
    return jnp.clip(drawn, min=-bound, max=bound).astype(kind)


def noise_with(own_key, extent, width, most, shards, heavy, kind=jnp.bfloat16):
    result = width * jax.random.normal(own_key, extent, jnp.float32)
    if shards:
        result = result * shard_levels(own_key, extent, shards, -0.22, 0.18)
    return jnp.clip(raised(result, jax.random.fold_in(own_key, 3), *heavy), -most, most).astype(kind)


def setup_inputs(seed: int = 0) -> dict:
    key_list = jax.random.split(jax.random.key(seed), 16)
    conv_out = bell_draw(key_list[0], (SEQUENCE_TOKENS, DR), 1.0, 6.0, ((0, 64), (1, 4)))
    gate_in = bell_draw(key_list[1], (SEQUENCE_TOKENS, DR), 1.0, 6.0, ((0, 64), (1, 4)))
    block_states = bell_draw(key_list[2], (N_SP, DR), 0.5, 4.0, ((0, 64), (1, 4)), jnp.float32)
    decay_param = draw_decay_param(jax.random.fold_in(key_list[15], 71), 0)
    decay_shift = draw_decay_shift(jax.random.fold_in(key_list[15], 71), 0)
    w_reset = bell_draw(key_list[5], (HEADS, HEAD_DIM, HEAD_DIM), HEAD_DIM ** -0.5, 0.5, ((0, 4),))
    w_input = bell_draw(key_list[6], (HEADS, HEAD_DIM, HEAD_DIM), HEAD_DIM ** -0.5, 0.5, ((0, 4),))
    w_out = bell_draw(key_list[7], (DR, D), DR ** -0.5, 0.125, ((0, 4),))
    mixed = bell_draw(key_list[8], (SEQUENCE_TOKENS, D), 1.0, 6.0, ((0, 64), (1, 4)))
    d_out = noise_with(key_list[9], (SEQUENCE_TOKENS, D), 1.0, 16.0, ((0, 64), (1, 4)), (0, 1, 64, 4.0))
    expert_ids_keys = jax.random.split(jax.random.fold_in(key_list[10], 1), SEQUENCE_TOKENS // TOK_DEV)
    expert_ids_turns = jax.random.permutation(jax.random.fold_in(key_list[10], 3), SEQUENCE_TOKENS // TOK_DEV)
    expert_ids = jax.vmap(lambda own, number: assign_block(jax.random.fold_in(key_list[10], 2), own, number, TOK_DEV, EXPERTS, TOP, CAP, 1))(expert_ids_keys, expert_ids_turns).reshape((SEQUENCE_TOKENS, TOP))
    route_weights = jnp.clip(0.2 + 1.19999997 * jax.random.uniform(key_list[11], (SEQUENCE_TOKENS, TOP), jnp.float32) ** shard_levels(key_list[11], (SEQUENCE_TOKENS, TOP), ((0, 64),), -0.2, 0.2), 0.2, 1.4)
    w_gate = bell_draw(key_list[12], (EXPERTS, D, FE), D ** -0.5, 0.125, ((0, 64), (2, 4)))
    w_up = bell_draw(key_list[13], (EXPERTS, D, FE), D ** -0.5, 0.125, ((0, 64), (2, 4)))
    w_down = bell_draw(key_list[14], (EXPERTS, FE, D), FE ** -0.5, 0.1875, ((0, 64), (1, 4)))
    return dict(conv_out=conv_out, gate_in=gate_in, block_states=block_states, decay_param=decay_param, decay_shift=decay_shift, w_reset=w_reset, w_input=w_input, w_out=w_out, mixed=mixed, d_out=d_out, expert_ids=expert_ids, route_weights=route_weights, w_gate=w_gate, w_up=w_up, w_down=w_down)


def decay_combine(first_pair, second_pair):
    return (first_pair[0] * second_pair[0], second_pair[0] * first_pair[1] + second_pair[1])

def gelu_slope(values):
    outcome, pullback = jax.vjp(jax.nn.gelu, values)
    return (outcome, pullback(jnp.ones_like(values))[0])

def head_maps(values, weights):
    count = values.shape[0]
    split = values.astype(jnp.float32).reshape(count, weights.shape[0], weights.shape[1])
    mapped = jnp.einsum('thi,hij->thj', split, weights.astype(jnp.float32))
    return mapped.reshape(count, -1)

def head_back(grads, weights):
    count = grads.shape[0]
    split = grads.astype(jnp.float32).reshape(count, weights.shape[0], weights.shape[2])
    mapped = jnp.einsum('thj,hij->thi', split, weights.astype(jnp.float32))
    return mapped.reshape(count, -1)

def over_rows(left_matrix, right_matrix):
    return lax.dot_general(left_matrix, right_matrix, (((0,), (0,)), ((), ())), preferred_element_type=jnp.float32)

def against_rows(left_matrix, right_matrix):
    return lax.dot_general(left_matrix, right_matrix, (((1,), (1,)), ((), ())), preferred_element_type=jnp.float32)

def reference(conv_out, gate_in, block_states, decay_param, decay_shift, w_reset, w_input, w_out, mixed, d_out, expert_ids, route_weights, w_gate, w_up, w_down):
    conv_full = conv_out.astype(jnp.float32)
    reset = jax.nn.sigmoid(head_maps(conv_out, w_reset))
    input_gate = jax.nn.sigmoid(head_maps(conv_out, w_input))
    slow_rate = jax.nn.softplus(-decay_param)
    log_decay = -8.0 * reset * slow_rate[None, :] + decay_shift[:, None]
    decays = jnp.exp(log_decay)
    norm_in = jnp.sqrt(-jnp.expm1(2.0 * log_decay))
    drives = norm_in * input_gate * conv_full
    blocked = (N_SP, TOK_DEV, DR)
    cum_decay, cum_drive = lax.associative_scan(decay_combine, (decays.reshape(blocked), drives.reshape(blocked)), axis=1)
    states = cum_decay * block_states[:, None, :] + cum_drive
    prev_states = jnp.concatenate([block_states[:, None, :], states[:, :-1]], axis=1).reshape(SEQUENCE_TOKENS, DR)
    states = states.reshape(SEQUENCE_TOKENS, DR)
    gate_act, gate_deriv = gelu_slope(gate_in.astype(jnp.float32))
    merged_in = (gate_act * states).astype(jnp.bfloat16)
    flat_ids = expert_ids.reshape(N_SP, TOK_DEV * TOP)
    onehot = (flat_ids[:, :, None] == jnp.arange(EXPERTS, dtype=jnp.int32)[None, None, :]).astype(jnp.int32)
    slot_rank = lax.optimization_barrier(jnp.sum((jnp.cumsum(onehot, axis=1) - 1) * onehot, axis=2))
    source_index = jnp.arange(N_SP, dtype=jnp.int32)[:, None]
    slot_flat = (source_index * CAP + slot_rank).reshape(-1).astype(jnp.int32)
    expert_flat = expert_ids.reshape(-1).astype(jnp.int32)
    assign_ids = jnp.arange(SEQUENCE_TOKENS * TOP, dtype=jnp.int32)
    slot_table = jnp.full((EXPERTS, N_SP * CAP), SEQUENCE_TOKENS * TOP, jnp.int32).at[expert_flat, slot_flat].set(assign_ids)
    scaled_cot = (route_weights[:, :, None] * d_out.astype(jnp.float32)[:, None, :]).astype(jnp.bfloat16).reshape(SEQUENCE_TOKENS * TOP, D)
    cot_padded = jnp.concatenate([scaled_cot, jnp.zeros((1, D), jnp.bfloat16)], axis=0)
    mixed_padded = jnp.concatenate([mixed, jnp.zeros((1, D), jnp.bfloat16)], axis=0)
    block_width = FE // N_TP

    def one_expert(operands):
        slot_ids, gate_matrix, up_matrix, down_matrix = operands
        token_ids = jnp.where(slot_ids < SEQUENCE_TOKENS * TOP, slot_ids // TOP, SEQUENCE_TOKENS)
        expert_in = mixed_padded[token_ids]
        expert_cot = cot_padded[slot_ids]
        up_pre = jnp.dot(expert_in, gate_matrix, preferred_element_type=jnp.float32)
        linear = jnp.dot(expert_in, up_matrix, preferred_element_type=jnp.float32)
        sigmoid_up = jax.nn.sigmoid(up_pre)
        silu_up = up_pre * sigmoid_up
        hidden_state = (silu_up * linear).astype(jnp.bfloat16)
        d_hidden = against_rows(expert_cot, down_matrix)
        d_linear = (d_hidden * silu_up).astype(jnp.bfloat16)
        d_up = (d_hidden * linear * sigmoid_up * (1.0 + up_pre * (1.0 - sigmoid_up))).astype(jnp.bfloat16)
        grad_gate_e = over_rows(expert_in, d_up)
        grad_up_e = over_rows(expert_in, d_linear)
        grad_down_e = over_rows(hidden_state, expert_cot)
        row_count = expert_in.shape[0]
        up_blocks = d_up.astype(jnp.float32).reshape(row_count, N_TP, block_width)
        lin_blocks = d_linear.astype(jnp.float32).reshape(row_count, N_TP, block_width)
        gate_blocks = gate_matrix.astype(jnp.float32).reshape(D, N_TP, block_width)
        upw_blocks = up_matrix.astype(jnp.float32).reshape(D, N_TP, block_width)
        pieces = jnp.einsum('rqf,dqf->qrd', up_blocks, gate_blocks) + jnp.einsum('rqf,dqf->qrd', lin_blocks, upw_blocks)
        rounded = lax.optimization_barrier(pieces.astype(jnp.bfloat16))
        row_grad = lax.optimization_barrier(jnp.sum(rounded.astype(jnp.float32), axis=0)).astype(jnp.bfloat16)
        return (grad_gate_e, grad_up_e, grad_down_e, row_grad)
    grad_w_gate, grad_w_up, grad_w_down, row_grads = lax.map(one_expert, (slot_table, w_gate, w_up, w_down))
    returned = row_grads[expert_flat, slot_flat].astype(jnp.float32).reshape(SEQUENCE_TOKENS, TOP, D)
    d_mixed = (d_out.astype(jnp.float32) + lax.optimization_barrier(jnp.sum(returned, axis=1))).astype(jnp.bfloat16)
    grad_out_proj_t = over_rows(d_mixed, merged_in)
    d_merged = against_rows(d_mixed, w_out)
    grad_gate = (d_merged * states * gate_deriv).astype(jnp.bfloat16)
    d_states = d_merged * gate_act
    next_decay = jnp.concatenate([decays[1:], jnp.zeros((1, DR), jnp.float32)], axis=0)
    _, state_flipped = lax.associative_scan(decay_combine, (next_decay[::-1], d_states[::-1]), axis=0)
    state_grad = state_flipped[::-1]
    d_log_decay = state_grad * decays * prev_states - state_grad * input_gate * conv_full * decays * decays / norm_in
    d_pre_reset = (d_log_decay * (-8.0 * slow_rate[None, :]) * reset * (1.0 - reset)).astype(jnp.bfloat16)
    d_pre_input = (state_grad * norm_in * conv_full * input_gate * (1.0 - input_gate)).astype(jnp.bfloat16)
    recurrence_input_gradient = (state_grad * norm_in * input_gate + head_back(d_pre_reset, w_reset) + head_back(d_pre_input, w_input)).astype(jnp.bfloat16)
    return (grad_w_gate, grad_w_up, grad_w_down, grad_out_proj_t, recurrence_input_gradient, grad_gate)
```

```python
import jax
import jax.numpy as jnp
import numpy as np
from jax import lax
from jax.experimental import pallas as pl
from jax.experimental.pallas import tpu as pltpu
from jax.sharding import Mesh
from jax.sharding import PartitionSpec as P

SP = ("z", "x", "c")
XC = ("x", "c")
F32 = jnp.float32
BF16 = jnp.bfloat16
VMEM = pl.BlockSpec(memory_space=pltpu.VMEM)
SMEM = pl.BlockSpec(memory_space=pltpu.SMEM)

TOK = 192
WIDTH = 512
EXPERTS = 64
CAP = 12
BLOCK = 2 * CAP
ROWS = EXPERTS * CAP
HALF = ROWS // 2
GROUP = 8 * BLOCK
GROUPS = EXPERTS * BLOCK // GROUP
HID = 256


def dot(a, b):
    return lax.dot_general(a, b, (((1,), (0,)), ((), ())), preferred_element_type=F32)


def dot_bt(a, b):
    return lax.dot_general(a, b, (((1,), (1,)), ((), ())), preferred_element_type=F32)


def dot_at(a, b):
    return lax.dot_general(a, b, (((0,), (0,)), ((), ())), preferred_element_type=F32)


def shape(dims, dtype):
    return jax.ShapeDtypeStruct(dims, dtype)


def local(kernel, name, outs, flops, *args, scratch=(), smem=0):
    moved = sum(a.size * a.dtype.itemsize for a in (*args, *jax.tree.leaves(outs)))
    return pl.pallas_call(
        kernel,
        name=name,
        out_shape=outs,
        in_specs=[SMEM] * smem + [VMEM] * (len(args) - smem),
        out_specs=jax.tree.map(lambda _: VMEM, outs),
        scratch_shapes=list(scratch),
        cost_estimate=pl.CostEstimate(flops=int(flops), bytes_accessed=moved, transcendentals=0),
    )(*args)


def shift(value, axis, by):
    n = lax.axis_size(axis)
    return lax.ppermute(value, axis, [(i, (i + by) % n) for i in range(n)])


def exchange(value, axes):
    return lax.all_to_all(value, axes, 0, 0, tiled=True)


def one_hot(mask):
    return jnp.where(mask, 1.0, 0.0).astype(BF16)


def route_kernel(ids_ref, ids_t_ref, weights_t_ref, mixed_ref, d_out_ref, send_ref, slots_ref):
    i32 = jnp.int32
    before = one_hot(
        lax.broadcasted_iota(i32, (TOK, TOK), 0) < lax.broadcasted_iota(i32, (TOK, TOK), 1)
    )
    expert = lax.broadcasted_iota(i32, (EXPERTS, TOK), 0)
    rows = [ids_t_ref[k : k + 1, :] for k in range(2)]
    named = [r == expert for r in rows]
    count = dot(one_hot(named[0] | named[1]), before)
    slot = [
        rows[k] * BLOCK
        + jnp.sum(jnp.where(named[k], count, 0.0), axis=0, keepdims=True).astype(i32)
        for k in range(2)
    ]
    later = one_hot(
        lax.broadcasted_iota(i32, (TOK, TOK), 1) < lax.broadcasted_iota(i32, (TOK, TOK), 0)
    )
    expert_c = lax.broadcasted_iota(i32, (TOK, EXPERTS), 1)
    cols = [ids_ref[:, k : k + 1] for k in range(2)]
    named_c = [c == expert_c for c in cols]
    count_c = dot(later, one_hot(named_c[0] | named_c[1]))
    for k in range(2):
        rank = jnp.sum(jnp.where(named_c[k], count_c, 0.0), axis=1, keepdims=True)
        slots_ref[:, k : k + 1] = cols[k] * BLOCK + rank.astype(i32)
    weights = [weights_t_ref[k : k + 1, :] for k in range(2)]
    mixed = mixed_ref[...]
    d_out = d_out_ref[...]

    def pack(g):
        at = lax.broadcasted_iota(i32, (GROUP, TOK), 0) + g * GROUP
        to_mix = one_hot((slot[0] == at) | (slot[1] == at))
        first, second = (slot[0] + CAP == at, slot[1] + CAP == at)
        to_cot = one_hot(first | second)
        scale = jnp.sum(
            jnp.where(first, weights[0], 0.0) + jnp.where(second, weights[1], 0.0),
            axis=1,
            keepdims=True,
        )
        value = dot(to_mix, mixed) + dot(to_cot, d_out) * scale
        send_ref[pl.ds(pl.multiple_of(g * GROUP, GROUP), GROUP), :] = value.astype(BF16)

    def two(n, carry):
        pack(2 * n)
        pack(2 * n + 1)
        return carry

    lax.fori_loop(0, GROUPS // 2, two, 0)


def sort_matrix():
    matrix = np.zeros((GROUP, GROUP), np.float32)
    for j in range(8):
        for r in range(CAP):
            matrix[j * CAP + r, j * BLOCK + r] = 1
            matrix[GROUP // 2 + j * CAP + r, j * BLOCK + CAP + r] = 1
    return jnp.asarray(matrix, BF16)


def spread_matrix():
    matrix = np.zeros((GROUP, GROUP // 2), np.float32)
    for j in range(8):
        for r in range(BLOCK):
            matrix[j * BLOCK + r, j * CAP + r % CAP] = 1
    return jnp.asarray(matrix, BF16)


def sort_kernel(got_ref, order_ref, mix_a, mix_b, cot_a, cot_b):
    order = order_ref[...]
    half = GROUP // 2
    for g in range(GROUPS):
        out = dot(order, got_ref[g * GROUP : (g + 1) * GROUP, :]).astype(BF16)
        at = (g % (GROUPS // 2)) * half
        mix, cot = (mix_a, cot_a) if g < GROUPS // 2 else (mix_b, cot_b)
        mix[at : at + half, :] = out[:half]
        cot[at : at + half, :] = out[half:]


def block_of(me_ref, step):
    return pl.multiple_of(((me_ref[0] + step) % 4) * WIDTH, WIDTH)


STEPS = (0, 3, 1, 2)


def expert_up_kernel(me_ref, *refs):
    pieces, (gate_ref, up_ref), (hidden_ref, silu_ref, slope_ref) = refs[:8], refs[8:10], refs[10:]
    for h in range(2):
        up_pre = linear = None
        for p in range(4):
            piece = pieces[2 * p + h][...]
            at = block_of(me_ref, STEPS[p])
            one = dot(piece, gate_ref[pl.ds(at, WIDTH), :])
            two = dot(piece, up_ref[pl.ds(at, WIDTH), :])
            up_pre = one if up_pre is None else up_pre + one
            linear = two if linear is None else linear + two
        sigmoid = jax.nn.sigmoid(up_pre)
        silu = up_pre * sigmoid
        rows = slice(h * HALF, (h + 1) * HALF)
        hidden_ref[rows, :] = (silu * linear).astype(BF16)
        silu_ref[rows, :] = silu
        slope_ref[rows, :] = linear * sigmoid * (1.0 + up_pre * (1.0 - sigmoid))


def expert_down_kernel(me_ref, *refs):
    pieces = refs[:8]
    gate_ref, up_ref, down_ref, silu_ref, slope_ref = refs[8:13]
    d_up_ref, d_linear_ref, far_a, far_b, left_ref, right_ref, own_ref = refs[13:]
    ups, linears = [], []
    for h in range(2):
        rows = slice(h * HALF, (h + 1) * HALF)
        d_hidden = None
        for p in range(4):
            at = block_of(me_ref, STEPS[p])
            one = dot_bt(pieces[2 * p + h][...], down_ref[:, pl.ds(at, WIDTH)])
            d_hidden = one if d_hidden is None else d_hidden + one
        d_linear_ref[rows, :] = (d_hidden * silu_ref[rows, :]).astype(BF16)
        d_up_ref[rows, :] = (d_hidden * slope_ref[rows, :]).astype(BF16)

    def part(rows, step):
        at = block_of(me_ref, step)
        return (
            dot_bt(d_up_ref[rows, :], gate_ref[pl.ds(at, WIDTH), :])
            + dot_bt(d_linear_ref[rows, :], up_ref[pl.ds(at, WIDTH), :])
        ).astype(BF16)

    top, low = (slice(0, HALF), slice(HALF, ROWS))
    far_a[...] = part(top, 2)
    far_b[...] = part(low, 2)
    for rows in (top, low):
        left_ref[rows, :] = part(rows, 3)
        right_ref[rows, :] = part(rows, 1)
        own_ref[rows, :] = part(rows, 0)


def expert_grad_kernel(me_ref, *refs):
    mixes, cots = refs[:8], refs[8:16]
    d_up_ref, d_linear_ref, hidden_ref = refs[16:19]
    grad_gate_ref, grad_up_ref, grad_down_ref = refs[19:]
    top, low = (slice(0, HALF), slice(HALF, ROWS))
    for p in range(4):
        mix = (mixes[2 * p], mixes[2 * p + 1])
        cot = (cots[2 * p], cots[2 * p + 1])

        def step(n, carry):
            cols = pl.ds(pl.multiple_of(n * 128, 128), 128)
            at = pl.ds(pl.multiple_of(block_of(me_ref, STEPS[p]) + n * 128, 128), 128)
            mix_a, mix_b = (mix[0][:, cols], mix[1][:, cols])
            grad_gate_ref[0, at, :] = dot_at(mix_a, d_up_ref[top, :]) + dot_at(
                mix_b, d_up_ref[low, :]
            )
            grad_up_ref[0, at, :] = dot_at(mix_a, d_linear_ref[top, :]) + dot_at(
                mix_b, d_linear_ref[low, :]
            )
            grad_down_ref[0, :, at] = dot_at(hidden_ref[top, :], cot[0][:, cols]) + dot_at(
                hidden_ref[low, :], cot[1][:, cols]
            )
            return carry

        lax.fori_loop(0, 4, step, 0)


def spread_kernel(own_ref, la_ref, lb_ref, ra_ref, rb_ref, order_ref, out_ref):
    order = order_ref[...]
    half = GROUP // 2
    first = (lax.broadcasted_iota(jnp.int32, (GROUP, 1), 0) % BLOCK) < CAP
    for g in range(GROUPS):
        at = (g % (GROUPS // 2)) * half
        from_left, from_right = (la_ref, ra_ref) if g < GROUPS // 2 else (lb_ref, rb_ref)
        total = (
            own_ref[g * half : (g + 1) * half, :].astype(F32)
            + from_left[at : at + half, :].astype(F32)
            + from_right[at : at + half, :].astype(F32)
        ).astype(BF16)
        wide = dot(order, total)
        out_ref[g * GROUP : (g + 1) * GROUP, :] = jnp.where(
            first, wide[:, : WIDTH // 2], wide[:, WIDTH // 2 :]
        ).astype(BF16)


def combine_kernel(back_ref, slots_ref, d_out_ref, out_ref, send_ref):
    at = lax.broadcasted_iota(jnp.int32, (TOK, EXPERTS * BLOCK), 1)
    one, two = (slots_ref[:, 0:1], slots_ref[:, 1:2])
    back = back_ref[...]
    for h in range(2):
        pick = one_hot((one + h * CAP == at) | (two + h * CAP == at))
        cols = slice(h * WIDTH // 2, (h + 1) * WIDTH // 2)
        out_ref[:, cols] = (d_out_ref[:, cols].astype(F32) + dot(pick, back)).astype(BF16)
    source = lax.broadcasted_iota(jnp.int32, (WIDTH, WIDTH), 0)
    target = lax.broadcasted_iota(jnp.int32, (WIDTH, WIDTH), 1)
    wanted = ((target >> 5) & 1) * 256 + (target >> 6) * 32 + (target & 31)
    moved = dot(out_ref[...], one_hot(source == wanted))
    lane = lax.broadcasted_iota(jnp.int32, (TOK // 2, 128), 1)
    for m in range(4):
        top = moved[: TOK // 2, 128 * m : 128 * (m + 1)]
        low = moved[TOK // 2 :, 128 * m : 128 * (m + 1)]
        send_ref[2 * m] = jnp.where(lane < 64, top, pltpu.roll(low, 64, 1)).astype(BF16)
        send_ref[2 * m + 1] = jnp.where(lane < 64, pltpu.roll(top, 64, 1), low).astype(BF16)


def neg_expm1(y):
    small = 1.0 + y * (1.0 / 7.0)
    for n in (6.0, 5.0, 4.0, 3.0, 2.0):
        small = 1.0 + y * small * (1.0 / n)
    return jnp.where(y > -0.5, -y * small, 1.0 - jnp.exp(y))


CHUNK = 16


def forward_kernel(
    conv_ref,
    gate_ref,
    start_ref,
    slow_ref,
    shift_ref,
    w_reset_ref,
    w_input_ref,
    merged_ref,
    act_ref,
    slope_ref,
    decay_ref,
    kr_ref,
    ki_ref,
    kd_ref,
    pre_r,
    pre_i,
):
    for h in range(4):
        cols = slice(h * 128, (h + 1) * 128)
        pre_r[:, cols] = dot(conv_ref[:, cols], w_reset_ref[h])
        pre_i[:, cols] = dot(conv_ref[:, cols], w_input_ref[h])
    row = lax.broadcasted_iota(jnp.int32, (8, WIDTH), 0)
    slow = -8.0 * slow_ref[...]

    def step(c, state):
        rows = pl.ds(pl.multiple_of(c * CHUNK, CHUNK), CHUNK)
        conv = conv_ref[rows, :].astype(F32)
        reset = jax.nn.sigmoid(pre_r[rows, :])
        gate_in = jax.nn.sigmoid(pre_i[rows, :])
        log_decay = reset * slow + shift_ref[rows, :]
        decay = jnp.exp(log_decay)
        norm = jnp.sqrt(neg_expm1(2.0 * log_decay))
        direct = norm * gate_in
        drive = direct * conv
        states, prevs = [], []
        for s in range(0, CHUNK, 8):
            a, b = (decay[s : s + 8], drive[s : s + 8])
            for d in (1, 2, 4):
                keep = row >= d
                b = jnp.where(keep, b + a * pltpu.roll(b, d, 0), b)
                a = jnp.where(keep, a * pltpu.roll(a, d, 0), a)
            now = a * state + b
            prevs.append(jnp.where(row == 0, state, pltpu.roll(now, 1, 0)))
            states.append(now)
            state = now[7:8, :]
        states = jnp.concatenate(states, axis=0)
        prevs = jnp.concatenate(prevs, axis=0)
        x = gate_ref[rows, :].astype(F32)
        c0 = 0.7978845608028654
        t = jnp.tanh(c0 * (x + 0.044715 * x * x * x))
        act = 0.5 * x * (1.0 + t)
        deriv = 0.5 * (1.0 + t) + 0.5 * x * (1.0 - t * t) * (c0 * (1.0 + 0.134145 * x * x))
        merged_ref[rows, :] = (act * states).astype(BF16)
        act_ref[rows, :] = act
        slope_ref[rows, :] = states * deriv
        decay_ref[rows, :] = decay
        d_log = decay * prevs - gate_in * conv * decay * decay / norm
        kr_ref[rows, :] = d_log * slow * reset * (1.0 - reset)
        ki_ref[rows, :] = drive * (1.0 - gate_in)
        kd_ref[rows, :] = direct
        return state

    lax.fori_loop(0, TOK // CHUNK, step, start_ref[...])


def project_kernel(me_ref, p0, p1, p2, p3, merged_ref, out_ref):
    half = TOK // 2
    top = merged_ref[:, :half, :].reshape(8 * half, WIDTH)
    low = merged_ref[:, half:, :].reshape(8 * half, WIDTH)
    for piece, step in zip((p0, p1, p2, p3), STEPS):
        at = pl.multiple_of(((me_ref[0] + step) % 4) * 64, 64)
        value = piece[...].reshape(8 * half, 128)
        total = dot_at(value, top)[:64] + dot_at(value, low)[64:]
        out_ref[pl.ds(at, 64), :] = total.astype(BF16)


def reverse_kernel(
    me_ref,
    p0,
    p1,
    p2,
    p3,
    w_out_ref,
    act_ref,
    slope_ref,
    decay_ref,
    grad_gate_ref,
    local_ref,
    prod_ref,
    carry_ref,
    merged_ref,
):
    total = None
    for piece, step in zip((p0, p1, p2, p3), STEPS):
        one = dot_bt(piece[...], w_out_ref[:, pl.ds(block_of(me_ref, step), WIDTH)])
        total = one if total is None else total + one
    merged_ref[...] = total
    row = lax.broadcasted_iota(jnp.int32, (8, WIDTH), 0)
    steps = TOK // 16

    def step(n, state):
        grad, prod, after = state
        at = pl.multiple_of((steps - 1 - n) * 16, 16)
        rows16 = pl.ds(at, 16)
        d_merged = merged_ref[rows16, :]
        grad_gate_ref[rows16, :] = (d_merged * slope_ref[rows16, :]).astype(BF16)
        d_states = d_merged * act_ref[rows16, :]
        decays = decay_ref[rows16, :]
        for s in (8, 0):
            decay = decays[s : s + 8]
            a = jnp.where(row == 7, after, pltpu.roll(decay, 7, 0))
            b = d_states[s : s + 8]
            for d in (1, 2, 4):
                keep = row < 8 - d
                b = jnp.where(keep, b + a * pltpu.roll(b, 8 - d, 0), b)
                a = jnp.where(keep, a * pltpu.roll(a, 8 - d, 0), a)
            now = b + a * grad
            products = a * prod
            rows8 = pl.ds(pl.multiple_of(at + s, 8), 8)
            local_ref[rows8, :] = now
            prod_ref[rows8, :] = products
            grad, prod, after = (now[0:1, :], products[0:1, :], decay[0:1, :])
        return (grad, prod, after)

    one = jnp.ones((1, WIDTH), F32)
    grad, prod, first = lax.fori_loop(0, steps, step, (jnp.zeros((1, WIDTH), F32), one, one))
    prod, lead = (prod * first, grad * first)
    rows = [prod[:, k * 128 : (k + 1) * 128] for k in range(4)]
    rows += [lead[:, k * 128 : (k + 1) * 128] for k in range(4)]
    tile = jnp.concatenate(rows, axis=0)
    for k in range(EXPERTS):
        carry_ref[8 * k : 8 * k + 8, :] = tile


def final_kernel(
    here_ref,
    carry_ref,
    local_ref,
    prod_ref,
    kr_ref,
    ki_ref,
    kd_ref,
    w_reset_ref,
    w_input_ref,
    out_ref,
):
    here = here_ref[0]

    def fold(n, value):
        source = EXPERTS - 1 - n
        tile = carry_ref[pl.ds(pl.multiple_of(source * 8, 8), 8), :]
        return tile[4:8] + tile[0:4] * value

    entering = lax.fori_loop(0, EXPERTS - 1 - here, fold, jnp.zeros((4, 128), F32))
    for h in range(4):
        cols = slice(h * 128, (h + 1) * 128)
        grad = local_ref[:, cols] + prod_ref[:, cols] * entering[h : h + 1, :]
        d_reset = (grad * kr_ref[:, cols]).astype(BF16)
        d_input = (grad * ki_ref[:, cols]).astype(BF16)
        out_ref[:, cols] = (
            grad * kd_ref[:, cols]
            + dot_bt(d_reset, w_reset_ref[h])
            + dot_bt(d_input, w_input_ref[h])
        ).astype(BF16)


def gathered(a, b):
    left_a, right_b = (shift(a, "tp", 1), shift(b, "tp", -1))
    left_b, right_a = (shift(b, "tp", 1), shift(a, "tp", -1))
    far_a, far_b = (shift(left_a, "tp", 1), shift(right_b, "tp", -1))
    return (a, b, left_a, left_b, right_a, right_b, far_a, far_b)


def collected(value):
    return (value, shift(value, "tp", 1), shift(value, "tp", -1), shift(value, "tp", 2))


def after(value, *others):
    return lax.optimization_barrier((value, others))[0]


def body(
    conv_out,
    gate_in,
    block_states,
    decay_param,
    decay_shift,
    w_reset,
    w_input,
    w_out,
    mixed,
    d_out,
    expert_ids,
    route_weights,
    w_gate,
    w_up,
    w_down,
):
    me = lax.axis_index("tp").astype(jnp.int32).reshape(1)
    here = lax.axis_index(SP).astype(jnp.int32).reshape(1)
    unit = 2 * ROWS * 2048 * HID
    send, slots = local(
        route_kernel,
        "route",
        (shape((EXPERTS * BLOCK, WIDTH), BF16), shape((TOK, 2), jnp.int32)),
        1.3e9,
        expert_ids,
        expert_ids.T,
        route_weights.T,
        mixed,
        d_out,
    )
    got = exchange(send, SP)
    f_like = shape((TOK, WIDTH), F32)
    slow_rate = jax.nn.softplus(-decay_param)
    merged, act, slope, decay, kr, ki, kd = local(
        forward_kernel,
        "forward",
        (shape((TOK, WIDTH), BF16),) + (f_like,) * 6,
        6e9,
        after(conv_out, send),
        gate_in,
        block_states,
        slow_rate.reshape(1, -1),
        decay_shift.reshape(-1, 1),
        w_reset,
        w_input,
        scratch=(pltpu.VMEM((TOK, WIDTH), F32),) * 2,
    )
    got = after(got, merged)
    piece = shape((HALF, WIDTH), BF16)
    mix_a, mix_b, cot_a, cot_b = local(
        sort_kernel, "sort", (piece,) * 4, 1e9, got, sort_matrix()
    )
    mixes = gathered(mix_a, mix_b)
    cots = gathered(cot_a, cot_b)
    gate2, up2, down2 = (w_gate[0], w_up[0], w_down[0])
    hid = shape((ROWS, HID), BF16)
    hid_f = shape((ROWS, HID), F32)
    full = shape((ROWS, WIDTH), BF16)
    hidden, silu, up_slope = local(
        expert_up_kernel, "expert_up", (hid, hid_f, hid_f), 2 * unit, me, *mixes, gate2, up2, smem=1
    )
    merged_x = exchange(jnp.broadcast_to(after(merged, hidden)[None], (8, TOK, WIDTH)), XC)
    d_up, d_linear, far_a, far_b, left, right, own = local(
        expert_down_kernel,
        "expert_down",
        (hid, hid, piece, piece, full, full, full),
        3 * unit,
        me,
        *cots,
        gate2,
        up2,
        down2,
        silu,
        up_slope,
        smem=1,
    )
    over_a, over_b = (shift(far_a, "tp", 1), shift(far_b, "tp", -1))
    right_b, left_a = (shift(right[HALF:], "tp", 1), shift(left[:HALF], "tp", -1))
    add = lambda u, v: (u.astype(F32) + v.astype(F32)).astype(BF16)
    right_a = shift(add(right[:HALF], over_a), "tp", 1)
    left_b = shift(add(left[HALF:], over_b), "tp", -1)
    returned = local(
        spread_kernel,
        "spread",
        shape((EXPERTS * BLOCK, WIDTH // 2), BF16),
        1e9,
        after(own, merged_x),
        right_a,
        right_b,
        left_a,
        left_b,
        spread_matrix(),
    )
    back = exchange(returned, SP)
    grads = local(
        expert_grad_kernel,
        "expert_grad",
        (shape((1, 2048, HID), F32), shape((1, 2048, HID), F32), shape((1, HID, 2048), F32)),
        3 * unit,
        me,
        *mixes,
        *cots,
        after(d_up, returned),
        d_linear,
        hidden,
        smem=1,
    )
    back = after(back, grads)
    d_columns, crossing = local(
        combine_kernel,
        "combine",
        (shape((TOK, WIDTH), BF16), shape((8, TOK // 2, 128), BF16)),
        1e9,
        back,
        slots,
        d_out,
    )
    crossed = exchange(crossing, XC)
    pieces = collected(d_columns)
    columns = collected(crossed)
    grad_gate, local_grad, products, carries = local(
        reverse_kernel,
        "reverse",
        (shape((TOK, WIDTH), BF16), f_like, f_like, shape((EXPERTS * 8, 128), F32)),
        4e9,
        me,
        after(pieces[0], crossed),
        *pieces[1:],
        w_out,
        act,
        slope,
        decay,
        scratch=(pltpu.VMEM((TOK, WIDTH), F32),),
        smem=1,
    )
    carried = exchange(carries, SP)
    grad_part = local(
        project_kernel,
        "project",
        shape((256, WIDTH), BF16),
        1e9,
        me,
        *columns,
        merged_x,
        smem=1,
    )
    parts = exchange(grad_part, "z")
    grad_out_proj_t = jnp.sum(parts.reshape(8, -1, WIDTH).astype(F32), axis=0)
    out = local(
        final_kernel,
        "final",
        shape((TOK, WIDTH), BF16),
        2e9,
        here,
        carried,
        local_grad,
        products,
        kr,
        ki,
        kd,
        w_reset,
        w_input,
        smem=1,
    )
    return (*grads, grad_out_proj_t, out, grad_gate)


def solution(mesh):
    torus = Mesh(mesh.devices.reshape(8, 4, 2, mesh.shape["tp"]), ("z", "x", "c", "tp"))
    in_specs = (
        P(SP, "tp"),
        P(SP, "tp"),
        P(SP, "tp"),
        P("tp"),
        P(SP),
        P("tp", None, None),
        P("tp", None, None),
        P("tp", None),
        P(SP, "tp"),
        P(SP, "tp"),
        P(SP, None),
        P(SP, None),
        P(SP, None, "tp"),
        P(SP, None, "tp"),
        P(SP, "tp", None),
    )
    out_specs = (
        P(SP, None, "tp"),
        P(SP, None, "tp"),
        P(SP, "tp", None),
        P(SP, "tp"),
        P(SP, "tp"),
        P(SP, "tp"),
    )
    return jax.shard_map(body, mesh=torus, in_specs=in_specs, out_specs=out_specs, check_vma=False)
```

```python
import jax
import jax.numpy as jnp
import numpy as np
from jax import lax
from jax.experimental import pallas as pl
from jax.experimental.pallas import tpu as pltpu
from jax.sharding import Mesh
from jax.sharding import PartitionSpec as P

SP = ("z", "x", "c")
XC = ("x", "c")
F32 = jnp.float32
BF16 = jnp.bfloat16
VMEM = pl.BlockSpec(memory_space=pltpu.VMEM)
SMEM = pl.BlockSpec(memory_space=pltpu.SMEM)

TOK = 192
WIDTH = 512
EXPERTS = 64
CAP = 12
BLOCK = 2 * CAP
SLOTS = EXPERTS * BLOCK
ROWS = 512
HALF = ROWS // 2
MORE = EXPERTS * CAP - ROWS
UNUSED = 256.0
WIDE = 384
PACKED = 4 * 2 * WIDTH + 3 * 256 + WIDTH
GROUP = 8 * BLOCK
GROUPS = EXPERTS * BLOCK // GROUP
HID = 256


def dot(a, b):
    return lax.dot_general(a, b, (((1,), (0,)), ((), ())), preferred_element_type=F32)


def dot_bt(a, b):
    return lax.dot_general(a, b, (((1,), (1,)), ((), ())), preferred_element_type=F32)


def dot_at(a, b):
    return lax.dot_general(a, b, (((0,), (0,)), ((), ())), preferred_element_type=F32)


def shape(dims, dtype):
    return jax.ShapeDtypeStruct(dims, dtype)


class Near:
    def __init__(self, value):
        self.value = value


def size(a):
    return a.size * a.dtype.itemsize


def local(kernel, name, outs, flops, *args, scratch=(), smem=0):
    def unwrapped(a):
        return a.value if isinstance(a, Near) else a

    def operand(n, a):
        if isinstance(a, Near):
            return pltpu.with_memory_space_constraint(a.value, pltpu.VMEM)
        if n < smem or a.ndim < 2:
            return a
        return pltpu.with_memory_space_constraint(a, pltpu.HBM)

    def result(o):
        if isinstance(o, Near):
            return pltpu.VMEM(o.value.shape, o.value.dtype)
        return pltpu.HBM(o.shape, o.dtype)

    single = not isinstance(outs, tuple)
    every = (*args, *((outs,) if single else outs))
    staged = sum(size(a) for a in every if not isinstance(a, Near))
    moved = sum(size(unwrapped(a)) for a in every)
    got = pl.pallas_call(
        kernel,
        name=name,
        out_shape=result(outs) if single else tuple(result(o) for o in outs),
        in_specs=[SMEM] * smem + [VMEM] * (len(args) - smem),
        out_specs=VMEM if single else (VMEM,) * len(outs),
        scratch_shapes=list(scratch),
        compiler_params=pltpu.CompilerParams(vmem_limit_bytes=staged + (10 << 20)),
        cost_estimate=pl.CostEstimate(flops=int(flops), bytes_accessed=moved, transcendentals=0),
    )(*[operand(n, a) for n, a in enumerate(args)])
    return got


def shift(value, axis, by):
    n = lax.axis_size(axis)
    return lax.ppermute(value, axis, [(i, (i + by) % n) for i in range(n)])


def exchange(value, axes):
    return lax.all_to_all(value, axes, 0, 0, tiled=True)


def one_hot(mask):
    return jnp.where(mask, 1.0, 0.0).astype(BF16)


def route_kernel(ids_ref, ids_t_ref, weights_t_ref, mixed_ref, d_out_ref, send_ref, slots_ref):
    i32 = jnp.int32
    before = one_hot(
        lax.broadcasted_iota(i32, (TOK, TOK), 0) < lax.broadcasted_iota(i32, (TOK, TOK), 1)
    )
    expert = lax.broadcasted_iota(i32, (EXPERTS, TOK), 0)
    rows = [ids_t_ref[k : k + 1, :] for k in range(2)]
    named = [r == expert for r in rows]
    count = dot(one_hot(named[0] | named[1]), before)
    slot = [
        rows[k] * BLOCK
        + jnp.sum(jnp.where(named[k], count, 0.0), axis=0, keepdims=True).astype(i32)
        for k in range(2)
    ]
    later = one_hot(
        lax.broadcasted_iota(i32, (TOK, TOK), 1) < lax.broadcasted_iota(i32, (TOK, TOK), 0)
    )
    expert_c = lax.broadcasted_iota(i32, (TOK, EXPERTS), 1)
    cols = [ids_ref[:, k : k + 1] for k in range(2)]
    named_c = [c == expert_c for c in cols]
    count_c = dot(later, one_hot(named_c[0] | named_c[1]))
    for k in range(2):
        rank = jnp.sum(jnp.where(named_c[k], count_c, 0.0), axis=1, keepdims=True)
        slots_ref[:, k : k + 1] = cols[k] * BLOCK + rank.astype(i32)
    weights = [weights_t_ref[k : k + 1, :] for k in range(2)]
    mixed = mixed_ref[...]
    d_out = d_out_ref[...]

    def pack(g, carry):
        at = lax.broadcasted_iota(i32, (GROUP, TOK), 0) + g * GROUP
        taken = (slot[0] == at) | (slot[1] == at)
        to_mix = one_hot(taken)
        empty = jnp.sum(jnp.where(taken, 1.0, 0.0), axis=1, keepdims=True) < 0.5
        empty &= (lax.broadcasted_iota(i32, (GROUP, 1), 0) % BLOCK) < CAP
        first, second = (slot[0] + CAP == at, slot[1] + CAP == at)
        to_cot = one_hot(first | second)
        scale = jnp.sum(
            jnp.where(first, weights[0], 0.0) + jnp.where(second, weights[1], 0.0),
            axis=1,
            keepdims=True,
        )
        value = dot(to_mix, mixed) + dot(to_cot, d_out) * scale + jnp.where(empty, UNUSED, 0.0)
        send_ref[pl.ds(pl.multiple_of(g * GROUP, GROUP), GROUP), :] = value.astype(BF16)
        return carry

    lax.fori_loop(0, GROUPS, pack, 0)


def sort_kernel(got_ref, rows_a, rows_b, place_ref, total_ref):
    i32 = jnp.int32
    before = lax.broadcasted_iota(i32, (WIDE, WIDE), 0)
    line = lax.broadcasted_iota(i32, (WIDE, WIDE), 1)
    slot = line - jnp.where(line % BLOCK >= CAP, CAP, 0)
    earlier, same = (one_hot(before < slot), one_hot(before == slot))
    first = (lax.broadcasted_iota(i32, (WIDE, 128), 0) % BLOCK) < CAP
    so_far = jnp.zeros((1, 128), F32)
    for g in range(SLOTS // WIDE):
        lines = slice(g * WIDE, (g + 1) * WIDE)
        used = one_hot(first & (got_ref[lines, :128].astype(F32) < UNUSED / 2))
        rank = dot_at(used, earlier)[0:1, :] + so_far[:, 0:1]
        held = dot_at(used, same)[0:1, :] > 0.5
        place_ref[:, lines] = jnp.where(held, rank, -1.0).astype(i32)
        so_far = so_far + jnp.sum(used.astype(F32), axis=0, keepdims=True)
    total_ref[...] = jnp.broadcast_to(so_far, (8, 128)).astype(i32)
    for n, rows in enumerate((rows_a, rows_b)):
        packed_rows(got_ref, place_ref, n * HALF, rows.at[:HALF], rows.at[HALF:])


def packed_rows(got_ref, place_ref, start, mix_ref, cot_ref):
    line = lax.broadcasted_iota(jnp.int32, (1, SLOTS), 1) % BLOCK
    place = place_ref[...]
    places = (jnp.where(line < CAP, place, -1), jnp.where(line < CAP, -1, place))

    def step(n, carry):
        row = lax.broadcasted_iota(jnp.int32, (128, SLOTS), 0) + (start + n * 128)
        rows = pl.ds(pl.multiple_of(n * 128, 128), 128)
        for wanted, out_ref in zip(places, (mix_ref, cot_ref)):
            out_ref[rows, :] = dot(one_hot(wanted == row), got_ref[...]).astype(BF16)
        return carry

    lax.fori_loop(0, mix_ref.shape[0] // 128, step, 0)


def sort_more_kernel(got_ref, place_ref, mix_ref, cot_ref):
    packed_rows(got_ref, place_ref, ROWS, mix_ref, cot_ref)


def block_of(me_ref, step):
    return pl.multiple_of(((me_ref[0] + step) % 4) * WIDTH, WIDTH)


STEPS = (0, 3, 1, 2)


def hidden_terms(me_ref, refs, turns, gate_ref, up_ref, down_ref, h):
    sums = None
    for p, turn in enumerate(turns):
        piece = refs[2 * p + h]
        at = block_of(me_ref, turn)
        mix = piece[:HALF, :]
        terms = (
            dot(mix, gate_ref[pl.ds(at, WIDTH), :]),
            dot(mix, up_ref[pl.ds(at, WIDTH), :]),
            dot_bt(piece[HALF:, :], down_ref[:, pl.ds(at, WIDTH)]),
        )
        sums = terms if sums is None else tuple(a + b for a, b in zip(sums, terms))
    return sums


def expert_near_kernel(me_ref, *refs):
    gate_ref, up_ref, down_ref = refs[6:9]
    for h in range(2):
        rows = slice(h * HALF, (h + 1) * HALF)
        terms = hidden_terms(me_ref, refs[:6], STEPS[:3], gate_ref, up_ref, down_ref, h)
        for term, out in zip(terms, refs[9:]):
            out[rows, :] = term


def expert_far_kernel(me_ref, *refs):
    gate_ref, up_ref, down_ref = refs[2:5]
    near_refs = refs[5:8]
    hidden_ref, d_up_ref, d_linear_ref, far_a, far_b, left_ref, right_ref, own_ref = refs[8:]
    for h in range(2):
        rows = slice(h * HALF, (h + 1) * HALF)
        terms = hidden_terms(me_ref, refs[:2], STEPS[3:], gate_ref, up_ref, down_ref, h)
        up_pre, linear, d_hidden = (a[rows, :] + b for a, b in zip(near_refs, terms))
        sigmoid = jax.nn.sigmoid(up_pre)
        silu = up_pre * sigmoid
        hidden_ref[rows, :] = (silu * linear).astype(BF16)
        d_linear_ref[rows, :] = (d_hidden * silu).astype(BF16)
        slope = linear * sigmoid * (1.0 + up_pre * (1.0 - sigmoid))
        d_up_ref[rows, :] = (d_hidden * slope).astype(BF16)

    def part(rows, turn):
        at = block_of(me_ref, turn)
        return (
            dot_bt(d_up_ref[rows, :], gate_ref[pl.ds(at, WIDTH), :])
            + dot_bt(d_linear_ref[rows, :], up_ref[pl.ds(at, WIDTH), :])
        ).astype(BF16)

    top, low = (slice(0, HALF), slice(HALF, ROWS))
    far_a[...] = part(top, 2)
    far_b[...] = part(low, 2)
    for rows in (top, low):
        left_ref[rows, :] = part(rows, 3)
        right_ref[rows, :] = part(rows, 1)
        own_ref[rows, :] = part(rows, 0)


def expert_grad_kernel(me_ref, total_ref, *refs):
    pieces = refs[:8]
    d_up_ref, d_linear_ref, hidden_ref, more_ref = refs[8:12]
    grad_gate_ref, grad_up_ref, grad_down_ref = refs[12:]
    top, low = (slice(0, HALF), slice(HALF, ROWS))
    for p in range(4):

        def step(n, carry, halves=(pieces[2 * p], pieces[2 * p + 1]), p=p):
            cols = pl.ds(pl.multiple_of(n * 128, 128), 128)
            at = pl.ds(pl.multiple_of(block_of(me_ref, STEPS[p]) + n * 128, 128), 128)
            mix_a, mix_b = (half[:HALF, cols] for half in halves)
            cot_a, cot_b = (half[HALF:, cols] for half in halves)
            grad_gate_ref[0, at, :] = dot_at(mix_a, d_up_ref[top, :]) + dot_at(
                mix_b, d_up_ref[low, :]
            )
            grad_up_ref[0, at, :] = dot_at(mix_a, d_linear_ref[top, :]) + dot_at(
                mix_b, d_linear_ref[low, :]
            )
            grad_down_ref[0, :, at] = dot_at(hidden_ref[top, :], cot_a) + dot_at(
                hidden_ref[low, :], cot_b
            )
            return carry

        lax.fori_loop(0, 4, step, 0)

    @pl.when(total_ref[0] > ROWS)
    def _():
        base = 8 * WIDTH
        d_up, d_linear, hidden = (more_ref[:, base + 256 * n : base + 256 * (n + 1)] for n in range(3))

        def step(n, carry):
            at = pl.ds(pl.multiple_of(n * 128, 128), 128)
            mix = more_ref[:, at]
            cot = more_ref[:, pl.ds(pl.multiple_of(n * 128 + 4 * WIDTH, 128), 128)]
            grad_gate_ref[0, at, :] += dot_at(mix, d_up)
            grad_up_ref[0, at, :] += dot_at(mix, d_linear)
            grad_down_ref[0, :, at] += dot_at(hidden, cot)
            return carry

        lax.fori_loop(0, 4 * WIDTH // 128, step, 0)


def spread_kernel(
    total_ref, own_ref, la_ref, lb_ref, ra_ref, rb_ref, place_ref, more_ref, out_ref
):
    rows = [
        (own.astype(F32) + from_left[...].astype(F32) + from_right[...].astype(F32)).astype(BF16)
        for own, from_left, from_right in (
            (own_ref[:HALF, :], la_ref, ra_ref),
            (own_ref[HALF:, :], lb_ref, rb_ref),
        )
    ]
    first = (lax.broadcasted_iota(jnp.int32, (WIDE, 1), 0) % BLOCK) < CAP

    def spread(values, start, lines):
        row = lax.broadcasted_iota(jnp.int32, (values.shape[0], WIDE), 0) + start
        wide = dot_at(one_hot(place_ref[:, lines] == row), values)
        return jnp.where(first, wide[:, : WIDTH // 2], wide[:, WIDTH // 2 :])

    def step(g, carry):
        lines = pl.ds(pl.multiple_of(g * WIDE, WIDE), WIDE)
        value = spread(rows[0], 0, lines) + spread(rows[1], HALF, lines)
        out_ref[lines, :] = value.astype(BF16)
        return carry

    lax.fori_loop(0, SLOTS // WIDE, step, 0)

    @pl.when(total_ref[0] > ROWS)
    def _():
        def add(g, carry):
            lines = pl.ds(pl.multiple_of(g * WIDE, WIDE), WIDE)
            value = spread(more_ref[:, PACKED - WIDTH :], ROWS, lines)
            out_ref[lines, :] = (out_ref[lines, :].astype(F32) + value).astype(BF16)
            return carry

        lax.fori_loop(0, SLOTS // WIDE, add, 0)


def combine_kernel(back_ref, slots_ref, d_out_ref, out_ref, send_ref):
    at = lax.broadcasted_iota(jnp.int32, (TOK, EXPERTS * BLOCK), 1)
    one, two = (slots_ref[:, 0:1], slots_ref[:, 1:2])
    back = back_ref[...]
    for h in range(2):
        pick = one_hot((one + h * CAP == at) | (two + h * CAP == at))
        cols = slice(h * WIDTH // 2, (h + 1) * WIDTH // 2)
        out_ref[:, cols] = (d_out_ref[:, cols].astype(F32) + dot(pick, back)).astype(BF16)
    source = lax.broadcasted_iota(jnp.int32, (WIDTH, WIDTH), 0)
    target = lax.broadcasted_iota(jnp.int32, (WIDTH, WIDTH), 1)
    wanted = ((target >> 5) & 1) * 256 + (target >> 6) * 32 + (target & 31)
    moved = dot(out_ref[...], one_hot(source == wanted))
    lane = lax.broadcasted_iota(jnp.int32, (TOK // 2, 128), 1)
    for m in range(4):
        top = moved[: TOK // 2, 128 * m : 128 * (m + 1)]
        low = moved[TOK // 2 :, 128 * m : 128 * (m + 1)]
        send_ref[2 * m] = jnp.where(lane < 64, top, pltpu.roll(low, 64, 1)).astype(BF16)
        send_ref[2 * m + 1] = jnp.where(lane < 64, pltpu.roll(top, 64, 1), low).astype(BF16)


def neg_expm1(y):
    small = 1.0 + y * (1.0 / 7.0)
    for n in (6.0, 5.0, 4.0, 3.0, 2.0):
        small = 1.0 + y * small * (1.0 / n)
    return jnp.where(y > -0.5, -y * small, 1.0 - jnp.exp(y))


CHUNK = 16


def forward_kernel(
    conv_ref,
    gate_ref,
    start_ref,
    slow_ref,
    shift_ref,
    w_reset_ref,
    w_input_ref,
    merged_ref,
    act_ref,
    slope_ref,
    decay_ref,
    kr_ref,
    ki_ref,
    kd_ref,
    pre_r,
    pre_i,
):
    for h in range(4):
        cols = slice(h * 128, (h + 1) * 128)
        pre_r[:, cols] = dot(conv_ref[:, cols], w_reset_ref[h])
        pre_i[:, cols] = dot(conv_ref[:, cols], w_input_ref[h])
    row = lax.broadcasted_iota(jnp.int32, (8, WIDTH), 0)
    slow = -8.0 * slow_ref[...]

    def step(c, state):
        rows = pl.ds(pl.multiple_of(c * CHUNK, CHUNK), CHUNK)
        conv = conv_ref[rows, :].astype(F32)
        reset = jax.nn.sigmoid(pre_r[rows, :])
        gate_in = jax.nn.sigmoid(pre_i[rows, :])
        log_decay = reset * slow + shift_ref[rows, :]
        decay = jnp.exp(log_decay)
        norm = jnp.sqrt(neg_expm1(2.0 * log_decay))
        direct = norm * gate_in
        drive = direct * conv
        states, prevs = [], []
        for s in range(0, CHUNK, 8):
            a, b = (decay[s : s + 8], drive[s : s + 8])
            for d in (1, 2, 4):
                keep = row >= d
                b = jnp.where(keep, b + a * pltpu.roll(b, d, 0), b)
                a = jnp.where(keep, a * pltpu.roll(a, d, 0), a)
            now = a * state + b
            prevs.append(jnp.where(row == 0, state, pltpu.roll(now, 1, 0)))
            states.append(now)
            state = now[7:8, :]
        states = jnp.concatenate(states, axis=0)
        prevs = jnp.concatenate(prevs, axis=0)
        x = gate_ref[rows, :].astype(F32)
        c0 = 0.7978845608028654
        t = jnp.tanh(c0 * (x + 0.044715 * x * x * x))
        act = 0.5 * x * (1.0 + t)
        deriv = 0.5 * (1.0 + t) + 0.5 * x * (1.0 - t * t) * (c0 * (1.0 + 0.134145 * x * x))
        merged = (act * states).astype(BF16)
        for k in range(8):
            merged_ref[k, rows, :] = merged
        act_ref[rows, :] = act
        slope_ref[rows, :] = states * deriv
        decay_ref[rows, :] = decay
        d_log = decay * prevs - gate_in * conv * decay * decay / norm
        kr_ref[rows, :] = d_log * slow * reset * (1.0 - reset)
        ki_ref[rows, :] = drive * (1.0 - gate_in)
        kd_ref[rows, :] = direct
        return state

    lax.fori_loop(0, TOK // CHUNK, step, start_ref[...])


def project_kernel(me_ref, p0, p1, p2, p3, merged_ref, out_ref):
    half = TOK // 2
    top = merged_ref[:, :half, :].reshape(8 * half, WIDTH)
    low = merged_ref[:, half:, :].reshape(8 * half, WIDTH)
    for piece, step in zip((p0, p1, p2, p3), STEPS):
        at = pl.multiple_of(((me_ref[0] + step) % 4) * 64, 64)
        value = piece[...].reshape(8 * half, 128)
        total = dot_at(value, top)[:64] + dot_at(value, low)[64:]
        out_ref[pl.ds(at, 64), :] = total.astype(BF16)


def reverse_kernel(
    me_ref,
    p0,
    p1,
    p2,
    p3,
    w_out_ref,
    act_ref,
    slope_ref,
    decay_ref,
    grad_gate_ref,
    local_ref,
    prod_ref,
    carry_ref,
    merged_ref,
):
    total = None
    for piece, step in zip((p0, p1, p2, p3), STEPS):
        one = dot_bt(piece[...], w_out_ref[:, pl.ds(block_of(me_ref, step), WIDTH)])
        total = one if total is None else total + one
    merged_ref[...] = total
    row = lax.broadcasted_iota(jnp.int32, (8, WIDTH), 0)
    steps = TOK // 16

    def step(n, state):
        grad, prod, after = state
        at = pl.multiple_of((steps - 1 - n) * 16, 16)
        rows16 = pl.ds(at, 16)
        d_merged = merged_ref[rows16, :]
        grad_gate_ref[rows16, :] = (d_merged * slope_ref[rows16, :]).astype(BF16)
        d_states = d_merged * act_ref[rows16, :]
        decays = decay_ref[rows16, :]
        for s in (8, 0):
            decay = decays[s : s + 8]
            a = jnp.where(row == 7, after, pltpu.roll(decay, 7, 0))
            b = d_states[s : s + 8]
            for d in (1, 2, 4):
                keep = row < 8 - d
                b = jnp.where(keep, b + a * pltpu.roll(b, 8 - d, 0), b)
                a = jnp.where(keep, a * pltpu.roll(a, 8 - d, 0), a)
            now = b + a * grad
            products = a * prod
            rows8 = pl.ds(pl.multiple_of(at + s, 8), 8)
            local_ref[rows8, :] = now
            prod_ref[rows8, :] = products
            grad, prod, after = (now[0:1, :], products[0:1, :], decay[0:1, :])
        return (grad, prod, after)

    one = jnp.ones((1, WIDTH), F32)
    grad, prod, first = lax.fori_loop(0, steps, step, (jnp.zeros((1, WIDTH), F32), one, one))
    prod, lead = (prod * first, grad * first)
    rows = [prod[:, k * 128 : (k + 1) * 128] for k in range(4)]
    rows += [lead[:, k * 128 : (k + 1) * 128] for k in range(4)]
    tile = jnp.concatenate(rows, axis=0)
    for k in range(EXPERTS):
        carry_ref[8 * k : 8 * k + 8, :] = tile


def final_kernel(
    here_ref,
    carry_ref,
    local_ref,
    prod_ref,
    kr_ref,
    ki_ref,
    kd_ref,
    w_reset_ref,
    w_input_ref,
    out_ref,
):
    here = here_ref[0]

    def fold(n, value):
        source = EXPERTS - 1 - n
        tile = carry_ref[pl.ds(pl.multiple_of(source * 8, 8), 8), :]
        return tile[4:8] + tile[0:4] * value

    entering = lax.fori_loop(0, EXPERTS - 1 - here, fold, jnp.zeros((4, 128), F32))
    for h in range(4):
        cols = slice(h * 128, (h + 1) * 128)
        grad = local_ref[:, cols] + prod_ref[:, cols] * entering[h : h + 1, :]
        d_reset = (grad * kr_ref[:, cols]).astype(BF16)
        d_input = (grad * ki_ref[:, cols]).astype(BF16)
        out_ref[:, cols] = (
            grad * kd_ref[:, cols]
            + dot_bt(d_reset, w_reset_ref[h])
            + dot_bt(d_input, w_input_ref[h])
        ).astype(BF16)


def gathered(a, b):
    left_a, right_b = (shift(a, "tp", 1), shift(b, "tp", -1))
    left_b, right_a = (shift(b, "tp", 1), shift(a, "tp", -1))
    far_a, far_b = (shift(left_a, "tp", 1), shift(right_b, "tp", -1))
    return (a, b, left_a, left_b, right_a, right_b, far_a, far_b)


def reduced(far_a, far_b, left, right):
    half = far_a.shape[0]

    def add(u, v):
        return (u.astype(F32) + v.astype(F32)).astype(BF16)

    over_a, over_b = (shift(far_a, "tp", 1), shift(far_b, "tp", -1))
    right_b, left_a = (shift(right[half:], "tp", 1), shift(left[:half], "tp", -1))
    right_a = shift(add(right[:half], over_a), "tp", 1)
    left_b = shift(add(left[half:], over_b), "tp", -1)
    return right_a, right_b, left_a, left_b, over_a


def overflow(gate2, up2, down2, got, place):
    full = shape((MORE, WIDTH), BF16)
    mix, cot = local(sort_more_kernel, "sort_more", (full, full), 1e9, got, place)
    both = exchange(jnp.broadcast_to(jnp.stack([mix, cot])[None], (4, 2, MORE, WIDTH)), "tp")
    mix, cot = (jnp.moveaxis(both[:, n], 0, 1).reshape(MORE, -1) for n in range(2))
    up_pre, linear = (dot(mix, gate2), dot(mix, up2))
    sigmoid = jax.nn.sigmoid(up_pre)
    silu = up_pre * sigmoid
    hidden = (silu * linear).astype(BF16)
    d_hidden = dot_bt(cot, down2)
    d_linear = (d_hidden * silu).astype(BF16)
    d_up = (d_hidden * (linear * sigmoid * (1.0 + up_pre * (1.0 - sigmoid)))).astype(BF16)
    part = (dot_bt(d_up, gate2) + dot_bt(d_linear, up2)).astype(BF16)
    parts = exchange(jnp.moveaxis(part.reshape(MORE, 4, WIDTH), 1, 0), "tp")
    total = jnp.sum(parts.astype(F32), axis=0).astype(BF16)
    return jnp.concatenate([mix, cot, d_up, d_linear, hidden, total], axis=1)


def collected(value):
    return (value, shift(value, "tp", 1), shift(value, "tp", -1), shift(value, "tp", 2))


def after(value, *others):
    return lax.optimization_barrier((value, others))[0]


def body(
    conv_out,
    gate_in,
    block_states,
    decay_param,
    decay_shift,
    w_reset,
    w_input,
    w_out,
    mixed,
    d_out,
    expert_ids,
    route_weights,
    w_gate,
    w_up,
    w_down,
):
    me = lax.axis_index("tp").astype(jnp.int32).reshape(1)
    here = lax.axis_index(SP).astype(jnp.int32).reshape(1)
    unit = 2 * ROWS * 2048 * HID
    send, slots = local(
        route_kernel,
        "route",
        (shape((EXPERTS * BLOCK, WIDTH), BF16), shape((TOK, 2), jnp.int32)),
        1.3e9,
        expert_ids,
        expert_ids.T,
        route_weights.T,
        mixed,
        d_out,
    )
    got = exchange(send, SP)
    f_like = shape((TOK, WIDTH), F32)
    slow_rate = jax.nn.softplus(-decay_param)
    merged, act, slope, decay, kr, ki, kd = local(
        forward_kernel,
        "forward",
        (shape((8, TOK, WIDTH), BF16),) + (f_like,) * 6,
        6e9,
        after(conv_out, send),
        gate_in,
        block_states,
        slow_rate.reshape(1, -1),
        decay_shift.reshape(-1, 1),
        w_reset,
        w_input,
        scratch=(pltpu.VMEM((TOK, WIDTH), F32),) * 2,
    )
    got = after(got, merged)
    piece = shape((HALF, WIDTH), BF16)
    full = shape((ROWS, WIDTH), BF16)
    rows_a, rows_b, place, total = local(
        sort_kernel,
        "sort",
        (Near(full), Near(full), shape((1, SLOTS), jnp.int32), shape((8, 128), jnp.int32)),
        2e9,
        Near(got),
    )
    total = total[0, :1]
    pieces = gathered(rows_a, rows_b)
    gate2, up2, down2 = (w_gate[0], w_up[0], w_down[0])
    hid = shape((ROWS, HID), BF16)
    hid_f = shape((ROWS, HID), F32)
    near = local(
        expert_near_kernel,
        "expert_near",
        (hid_f,) * 3,
        2 * unit,
        me,
        *map(Near, pieces[:6]),
        gate2,
        up2,
        down2,
        smem=1,
    )
    merged_x = exchange(after(merged, pieces[3]), XC)
    hidden, d_up, d_linear, far_a, far_b, left, right, own = local(
        expert_far_kernel,
        "expert_far",
        (hid, hid, hid, *map(Near, (piece, piece, full, full)), full),
        3 * unit,
        me,
        *map(Near, pieces[6:]),
        gate2,
        up2,
        down2,
        *near,
        smem=1,
    )
    right_a, right_b, left_a, left_b, over_a = reduced(far_a, far_b, left, right)
    more = lax.cond(
        total[0] > ROWS,
        lambda *both: overflow(gate2, up2, down2, *both),
        lambda *_: jnp.zeros((MORE, PACKED), BF16),
        after(got, pieces[2]),
        place,
    )
    returned = local(
        spread_kernel,
        "spread",
        shape((EXPERTS * BLOCK, WIDTH // 2), BF16),
        2e9,
        total,
        after(own, merged_x),
        Near(right_a),
        Near(right_b),
        Near(left_a),
        Near(left_b),
        place,
        more,
        smem=1,
    )
    back = exchange(returned, SP)
    grads = local(
        expert_grad_kernel,
        "expert_grad",
        (shape((1, 2048, HID), F32), shape((1, 2048, HID), F32), shape((1, HID, 2048), F32)),
        3 * unit,
        me,
        total,
        *pieces,
        after(d_up, returned),
        d_linear,
        hidden,
        more,
        smem=2,
    )
    back = after(back, grads)
    d_columns, crossing = local(
        combine_kernel,
        "combine",
        (Near(shape((TOK, WIDTH), BF16)), Near(shape((8, TOK // 2, 128), BF16))),
        1e9,
        Near(back),
        slots,
        d_out,
    )
    crossed = exchange(crossing, XC)
    pieces = collected(d_columns)
    columns = collected(crossed)
    grad_gate, local_grad, products, carries = local(
        reverse_kernel,
        "reverse",
        (shape((TOK, WIDTH), BF16), Near(f_like), Near(f_like), shape((EXPERTS * 8, 128), F32)),
        4e9,
        me,
        *map(Near, (after(pieces[0], crossed), *pieces[1:])),
        w_out,
        act,
        slope,
        decay,
        scratch=(pltpu.VMEM((TOK, WIDTH), F32),),
        smem=1,
    )
    carried = exchange(carries, SP)
    grad_part = local(
        project_kernel,
        "project",
        shape((256, WIDTH), BF16),
        1e9,
        me,
        *map(Near, columns),
        Near(merged_x),
        smem=1,
    )
    parts = exchange(grad_part, "z")
    grad_out_proj_t = jnp.sum(parts.reshape(8, -1, WIDTH).astype(F32), axis=0)
    out = local(
        final_kernel,
        "final",
        shape((TOK, WIDTH), BF16),
        2e9,
        here,
        Near(carried),
        Near(local_grad),
        Near(products),
        kr,
        ki,
        kd,
        w_reset,
        w_input,
        smem=1,
    )
    return (*grads, grad_out_proj_t, out, grad_gate)


def solution(mesh):
    torus = Mesh(mesh.devices.reshape(8, 4, 2, mesh.shape["tp"]), ("z", "x", "c", "tp"))
    in_specs = (
        P(SP, "tp"),
        P(SP, "tp"),
        P(SP, "tp"),
        P("tp"),
        P(SP),
        P("tp", None, None),
        P("tp", None, None),
        P("tp", None),
        P(SP, "tp"),
        P(SP, "tp"),
        P(SP, None),
        P(SP, None),
        P(SP, None, "tp"),
        P(SP, None, "tp"),
        P(SP, "tp", None),
    )
    out_specs = (
        P(SP, None, "tp"),
        P(SP, None, "tp"),
        P(SP, "tp", None),
        P(SP, "tp"),
        P(SP, "tp"),
        P(SP, "tp"),
    )
    return jax.shard_map(body, mesh=torus, in_specs=in_specs, out_specs=out_specs, check_vma=False)
```

```python
import jax
import jax.numpy as jnp
import numpy as np
from jax import lax
from jax.experimental import pallas as pl
from jax.experimental.pallas import tpu as pltpu
from jax.sharding import Mesh
from jax.sharding import PartitionSpec as P

SP = ("z", "x", "c")
XC = ("x", "c")
F32 = jnp.float32
BF16 = jnp.bfloat16
VMEM = pl.BlockSpec(memory_space=pltpu.VMEM)
SMEM = pl.BlockSpec(memory_space=pltpu.SMEM)

TOK = 192
WIDTH = 512
EXPERTS = 64
CAP = 12
BLOCK = 2 * CAP
ROWS = EXPERTS * CAP
HALF = ROWS // 2
GROUP = 8 * BLOCK
GROUPS = EXPERTS * BLOCK // GROUP
HID = 256


def dot(a, b):
    return lax.dot_general(a, b, (((1,), (0,)), ((), ())), preferred_element_type=F32)


def dot_bt(a, b):
    return lax.dot_general(a, b, (((1,), (1,)), ((), ())), preferred_element_type=F32)


def dot_at(a, b):
    return lax.dot_general(a, b, (((0,), (0,)), ((), ())), preferred_element_type=F32)


def shape(dims, dtype):
    return jax.ShapeDtypeStruct(dims, dtype)


class Near:
    def __init__(self, value):
        self.value = value


def size(a):
    return a.size * a.dtype.itemsize


def local(kernel, name, outs, flops, *args, scratch=(), smem=0):
    def unwrapped(a):
        return a.value if isinstance(a, Near) else a

    def operand(n, a):
        if isinstance(a, Near):
            return pltpu.with_memory_space_constraint(a.value, pltpu.VMEM)
        if n < smem or a.ndim < 2:
            return a
        return pltpu.with_memory_space_constraint(a, pltpu.HBM)

    def result(o):
        if isinstance(o, Near):
            return pltpu.VMEM(o.value.shape, o.value.dtype)
        return pltpu.HBM(o.shape, o.dtype)

    single = not isinstance(outs, tuple)
    every = (*args, *((outs,) if single else outs))
    staged = sum(size(a) for a in every if not isinstance(a, Near))
    moved = sum(size(unwrapped(a)) for a in every)
    got = pl.pallas_call(
        kernel,
        name=name,
        out_shape=result(outs) if single else tuple(result(o) for o in outs),
        in_specs=[SMEM] * smem + [VMEM] * (len(args) - smem),
        out_specs=VMEM if single else (VMEM,) * len(outs),
        scratch_shapes=list(scratch),
        compiler_params=pltpu.CompilerParams(vmem_limit_bytes=staged + (10 << 20)),
        cost_estimate=pl.CostEstimate(flops=int(flops), bytes_accessed=moved, transcendentals=0),
    )(*[operand(n, a) for n, a in enumerate(args)])
    return got


def shift(value, axis, by):
    n = lax.axis_size(axis)
    return lax.ppermute(value, axis, [(i, (i + by) % n) for i in range(n)])


def exchange(value, axes):
    return lax.all_to_all(value, axes, 0, 0, tiled=True)


def one_hot(mask):
    return jnp.where(mask, 1.0, 0.0).astype(BF16)


def slots_kernel(ids_ref, slots_ref):
    i32 = jnp.int32
    later = one_hot(
        lax.broadcasted_iota(i32, (TOK, TOK), 1) < lax.broadcasted_iota(i32, (TOK, TOK), 0)
    )
    expert_c = lax.broadcasted_iota(i32, (TOK, EXPERTS), 1)
    cols = [ids_ref[:, k : k + 1] for k in range(2)]
    named_c = [c == expert_c for c in cols]
    count_c = dot(later, one_hot(named_c[0] | named_c[1]))
    for k in range(2):
        rank = jnp.sum(jnp.where(named_c[k], count_c, 0.0), axis=1, keepdims=True)
        slots_ref[:, k : k + 1] = cols[k] * BLOCK + rank.astype(i32)


def route_kernel(ids_t_ref, weights_t_ref, mixed_ref, d_out_ref, send_ref):
    i32 = jnp.int32
    before = one_hot(
        lax.broadcasted_iota(i32, (TOK, TOK), 0) < lax.broadcasted_iota(i32, (TOK, TOK), 1)
    )
    expert = lax.broadcasted_iota(i32, (EXPERTS, TOK), 0)
    rows = [ids_t_ref[k : k + 1, :] for k in range(2)]
    named = [r == expert for r in rows]
    count = dot(one_hot(named[0] | named[1]), before)
    slot = [
        rows[k] * BLOCK
        + jnp.sum(jnp.where(named[k], count, 0.0), axis=0, keepdims=True).astype(i32)
        for k in range(2)
    ]
    weights = [weights_t_ref[k : k + 1, :] for k in range(2)]
    mixed = mixed_ref[...]
    d_out = d_out_ref[...]

    def pack(g):
        at = lax.broadcasted_iota(i32, (GROUP, TOK), 0) + g * GROUP
        to_mix = one_hot((slot[0] == at) | (slot[1] == at))
        first, second = (slot[0] + CAP == at, slot[1] + CAP == at)
        to_cot = one_hot(first | second)
        scale = jnp.sum(
            jnp.where(first, weights[0], 0.0) + jnp.where(second, weights[1], 0.0),
            axis=1,
            keepdims=True,
        )
        value = dot(to_mix, mixed) + dot(to_cot, d_out) * scale
        send_ref[pl.ds(pl.multiple_of(g * GROUP, GROUP), GROUP), :] = value.astype(BF16)

    def two(n, carry):
        pack(2 * n)
        pack(2 * n + 1)
        return carry

    lax.fori_loop(0, GROUPS // 2, two, 0)


def sort_matrix():
    matrix = np.zeros((GROUP, GROUP), np.float32)
    for j in range(8):
        for r in range(CAP):
            matrix[j * CAP + r, j * BLOCK + r] = 1
            matrix[GROUP // 2 + j * CAP + r, j * BLOCK + CAP + r] = 1
    return jnp.asarray(matrix, BF16)


def spread_matrix():
    matrix = np.zeros((GROUP, GROUP // 2), np.float32)
    for j in range(8):
        for r in range(BLOCK):
            matrix[j * BLOCK + r, j * CAP + r % CAP] = 1
    return jnp.asarray(matrix, BF16)


def sort_kernel(got_ref, order_ref, rows_a, rows_b):
    order = order_ref[...]
    half = GROUP // 2
    for g in range(GROUPS):
        out = dot(order, got_ref[g * GROUP : (g + 1) * GROUP, :]).astype(BF16)
        at = (g % (GROUPS // 2)) * half
        rows = rows_a if g < GROUPS // 2 else rows_b
        rows[at : at + half, :] = out[:half]
        rows[HALF + at : HALF + at + half, :] = out[half:]


def block_of(me_ref, step):
    return pl.multiple_of(((me_ref[0] + step) % 4) * WIDTH, WIDTH)


STEPS = (0, 3, 1, 2)


def hidden_terms(me_ref, refs, turns, gate_ref, up_ref, down_ref, h):
    sums = None
    for p, turn in enumerate(turns):
        piece = refs[2 * p + h]
        at = block_of(me_ref, turn)
        mix = piece[:HALF, :]
        terms = (
            dot(mix, gate_ref[pl.ds(at, WIDTH), :]),
            dot(mix, up_ref[pl.ds(at, WIDTH), :]),
            dot_bt(piece[HALF:, :], down_ref[:, pl.ds(at, WIDTH)]),
        )
        sums = terms if sums is None else tuple(a + b for a, b in zip(sums, terms))
    return sums


def expert_near_kernel(me_ref, *refs):
    gate_ref, up_ref, down_ref = refs[6:9]
    for h in range(2):
        rows = slice(h * HALF, (h + 1) * HALF)
        terms = hidden_terms(me_ref, refs[:6], STEPS[:3], gate_ref, up_ref, down_ref, h)
        for term, out in zip(terms, refs[9:]):
            out[rows, :] = term


def expert_far_kernel(me_ref, *refs):
    gate_ref, up_ref, down_ref = refs[2:5]
    near_refs = refs[5:8]
    hidden_ref, d_up_ref, d_linear_ref, far_a, far_b, left_ref, right_ref, own_ref = refs[8:]
    for h in range(2):
        rows = slice(h * HALF, (h + 1) * HALF)
        terms = hidden_terms(me_ref, refs[:2], STEPS[3:], gate_ref, up_ref, down_ref, h)
        up_pre, linear, d_hidden = (a[rows, :] + b for a, b in zip(near_refs, terms))
        sigmoid = jax.nn.sigmoid(up_pre)
        silu = up_pre * sigmoid
        hidden_ref[rows, :] = (silu * linear).astype(BF16)
        d_linear_ref[rows, :] = (d_hidden * silu).astype(BF16)
        slope = linear * sigmoid * (1.0 + up_pre * (1.0 - sigmoid))
        d_up_ref[rows, :] = (d_hidden * slope).astype(BF16)

    def part(rows, turn):
        at = block_of(me_ref, turn)
        return (
            dot_bt(d_up_ref[rows, :], gate_ref[pl.ds(at, WIDTH), :])
            + dot_bt(d_linear_ref[rows, :], up_ref[pl.ds(at, WIDTH), :])
        ).astype(BF16)

    top, low = (slice(0, HALF), slice(HALF, ROWS))
    far_a[...] = part(top, 2)
    far_b[...] = part(low, 2)
    for rows in (top, low):
        left_ref[rows, :] = part(rows, 3)
        right_ref[rows, :] = part(rows, 1)
        own_ref[rows, :] = part(rows, 0)


def expert_grad_kernel(me_ref, *refs):
    pieces = refs[:8]
    d_up_ref, d_linear_ref, hidden_ref = refs[8:11]
    grad_gate_ref, grad_up_ref, grad_down_ref = refs[11:]
    top, low = (slice(0, HALF), slice(HALF, ROWS))
    for p in range(4):

        def step(n, carry, halves=(pieces[2 * p], pieces[2 * p + 1]), p=p):
            cols = pl.ds(pl.multiple_of(n * 128, 128), 128)
            at = pl.ds(pl.multiple_of(block_of(me_ref, STEPS[p]) + n * 128, 128), 128)
            mix_a, mix_b = (half[:HALF, cols] for half in halves)
            cot_a, cot_b = (half[HALF:, cols] for half in halves)
            grad_gate_ref[0, at, :] = dot_at(mix_a, d_up_ref[top, :]) + dot_at(
                mix_b, d_up_ref[low, :]
            )
            grad_up_ref[0, at, :] = dot_at(mix_a, d_linear_ref[top, :]) + dot_at(
                mix_b, d_linear_ref[low, :]
            )
            grad_down_ref[0, :, at] = dot_at(hidden_ref[top, :], cot_a) + dot_at(
                hidden_ref[low, :], cot_b
            )
            return carry

        lax.fori_loop(0, 4, step, 0)


def spread_kernel(own_ref, la_ref, lb_ref, ra_ref, rb_ref, order_ref, out_ref):
    order = order_ref[...]
    half = GROUP // 2
    first = (lax.broadcasted_iota(jnp.int32, (GROUP, 1), 0) % BLOCK) < CAP
    for g in range(GROUPS):
        at = (g % (GROUPS // 2)) * half
        from_left, from_right = (la_ref, ra_ref) if g < GROUPS // 2 else (lb_ref, rb_ref)
        total = (
            own_ref[g * half : (g + 1) * half, :].astype(F32)
            + from_left[at : at + half, :].astype(F32)
            + from_right[at : at + half, :].astype(F32)
        ).astype(BF16)
        wide = dot(order, total)
        out_ref[g * GROUP : (g + 1) * GROUP, :] = jnp.where(
            first, wide[:, : WIDTH // 2], wide[:, WIDTH // 2 :]
        ).astype(BF16)


def combine_kernel(back_ref, slots_ref, d_out_ref, out_ref, send_ref):
    at = lax.broadcasted_iota(jnp.int32, (TOK, EXPERTS * BLOCK), 1)
    one, two = (slots_ref[:, 0:1], slots_ref[:, 1:2])
    back = back_ref[...]
    for h in range(2):
        pick = one_hot((one + h * CAP == at) | (two + h * CAP == at))
        cols = slice(h * WIDTH // 2, (h + 1) * WIDTH // 2)
        out_ref[:, cols] = (d_out_ref[:, cols].astype(F32) + dot(pick, back)).astype(BF16)
    source = lax.broadcasted_iota(jnp.int32, (WIDTH, WIDTH), 0)
    target = lax.broadcasted_iota(jnp.int32, (WIDTH, WIDTH), 1)
    wanted = ((target >> 5) & 1) * 256 + (target >> 6) * 32 + (target & 31)
    moved = dot(out_ref[...], one_hot(source == wanted))
    lane = lax.broadcasted_iota(jnp.int32, (TOK // 2, 128), 1)
    for m in range(4):
        top = moved[: TOK // 2, 128 * m : 128 * (m + 1)]
        low = moved[TOK // 2 :, 128 * m : 128 * (m + 1)]
        send_ref[2 * m] = jnp.where(lane < 64, top, pltpu.roll(low, 64, 1)).astype(BF16)
        send_ref[2 * m + 1] = jnp.where(lane < 64, pltpu.roll(top, 64, 1), low).astype(BF16)


def neg_expm1(y):
    small = 1.0 + y * (1.0 / 7.0)
    for n in (6.0, 5.0, 4.0, 3.0, 2.0):
        small = 1.0 + y * small * (1.0 / n)
    return jnp.where(y > -0.5, -y * small, 1.0 - jnp.exp(y))


CHUNK = 16


def forward_kernel(
    conv_ref,
    gate_ref,
    start_ref,
    slow_ref,
    shift_ref,
    w_reset_ref,
    w_input_ref,
    merged_ref,
    act_ref,
    slope_ref,
    decay_ref,
    kr_ref,
    ki_ref,
    kd_ref,
    pre_r,
    pre_i,
):
    for h in range(4):
        cols = slice(h * 128, (h + 1) * 128)
        pre_r[:, cols] = dot(conv_ref[:, cols], w_reset_ref[h])
        pre_i[:, cols] = dot(conv_ref[:, cols], w_input_ref[h])
    row = lax.broadcasted_iota(jnp.int32, (8, WIDTH), 0)
    slow = -8.0 * slow_ref[...]

    def step(c, state):
        rows = pl.ds(pl.multiple_of(c * CHUNK, CHUNK), CHUNK)
        conv = conv_ref[rows, :].astype(F32)
        reset = jax.nn.sigmoid(pre_r[rows, :])
        gate_in = jax.nn.sigmoid(pre_i[rows, :])
        log_decay = reset * slow + shift_ref[rows, :]
        decay = jnp.exp(log_decay)
        norm = jnp.sqrt(neg_expm1(2.0 * log_decay))
        direct = norm * gate_in
        drive = direct * conv
        states, prevs = [], []
        for s in range(0, CHUNK, 8):
            a, b = (decay[s : s + 8], drive[s : s + 8])
            for d in (1, 2, 4):
                keep = row >= d
                b = jnp.where(keep, b + a * pltpu.roll(b, d, 0), b)
                a = jnp.where(keep, a * pltpu.roll(a, d, 0), a)
            now = a * state + b
            prevs.append(jnp.where(row == 0, state, pltpu.roll(now, 1, 0)))
            states.append(now)
            state = now[7:8, :]
        states = jnp.concatenate(states, axis=0)
        prevs = jnp.concatenate(prevs, axis=0)
        x = gate_ref[rows, :].astype(F32)
        c0 = 0.7978845608028654
        t = jnp.tanh(c0 * (x + 0.044715 * x * x * x))
        act = 0.5 * x * (1.0 + t)
        deriv = 0.5 * (1.0 + t) + 0.5 * x * (1.0 - t * t) * (c0 * (1.0 + 0.134145 * x * x))
        merged = (act * states).astype(BF16)
        for k in range(8):
            merged_ref[k, rows, :] = merged
        act_ref[rows, :] = act
        slope_ref[rows, :] = states * deriv
        decay_ref[rows, :] = decay
        d_log = decay * prevs - gate_in * conv * decay * decay / norm
        kr_ref[rows, :] = d_log * slow * reset * (1.0 - reset)
        ki_ref[rows, :] = drive * (1.0 - gate_in)
        kd_ref[rows, :] = direct
        return state

    lax.fori_loop(0, TOK // CHUNK, step, start_ref[...])


def project_kernel(me_ref, p0, p1, p2, p3, merged_ref, out_ref):
    half = TOK // 2
    top = merged_ref[:, :half, :].reshape(8 * half, WIDTH)
    low = merged_ref[:, half:, :].reshape(8 * half, WIDTH)
    for piece, step in zip((p0, p1, p2, p3), STEPS):
        at = pl.multiple_of(((me_ref[0] + step) % 4) * 64, 64)
        value = piece[...].reshape(8 * half, 128)
        total = dot_at(value, top)[:64] + dot_at(value, low)[64:]
        out_ref[pl.ds(at, 64), :] = total.astype(BF16)


def reverse_kernel(
    me_ref,
    p0,
    p1,
    p2,
    p3,
    w_out_ref,
    act_ref,
    slope_ref,
    decay_ref,
    grad_gate_ref,
    local_ref,
    prod_ref,
    carry_ref,
    merged_ref,
):
    total = None
    for piece, step in zip((p0, p1, p2, p3), STEPS):
        one = dot_bt(piece[...], w_out_ref[:, pl.ds(block_of(me_ref, step), WIDTH)])
        total = one if total is None else total + one
    merged_ref[...] = total
    row = lax.broadcasted_iota(jnp.int32, (8, WIDTH), 0)
    steps = TOK // 16

    def step(n, state):
        grad, prod, after = state
        at = pl.multiple_of((steps - 1 - n) * 16, 16)
        rows16 = pl.ds(at, 16)
        d_merged = merged_ref[rows16, :]
        grad_gate_ref[rows16, :] = (d_merged * slope_ref[rows16, :]).astype(BF16)
        d_states = d_merged * act_ref[rows16, :]
        decays = decay_ref[rows16, :]
        for s in (8, 0):
            decay = decays[s : s + 8]
            a = jnp.where(row == 7, after, pltpu.roll(decay, 7, 0))
            b = d_states[s : s + 8]
            for d in (1, 2, 4):
                keep = row < 8 - d
                b = jnp.where(keep, b + a * pltpu.roll(b, 8 - d, 0), b)
                a = jnp.where(keep, a * pltpu.roll(a, 8 - d, 0), a)
            now = b + a * grad
            products = a * prod
            rows8 = pl.ds(pl.multiple_of(at + s, 8), 8)
            local_ref[rows8, :] = now
            prod_ref[rows8, :] = products
            grad, prod, after = (now[0:1, :], products[0:1, :], decay[0:1, :])
        return (grad, prod, after)

    one = jnp.ones((1, WIDTH), F32)
    grad, prod, first = lax.fori_loop(0, steps, step, (jnp.zeros((1, WIDTH), F32), one, one))
    prod, lead = (prod * first, grad * first)
    rows = [prod[:, k * 128 : (k + 1) * 128] for k in range(4)]
    rows += [lead[:, k * 128 : (k + 1) * 128] for k in range(4)]
    tile = jnp.concatenate(rows, axis=0)
    for k in range(EXPERTS):
        carry_ref[8 * k : 8 * k + 8, :] = tile


def final_kernel(
    here_ref,
    carry_ref,
    local_ref,
    prod_ref,
    kr_ref,
    ki_ref,
    kd_ref,
    w_reset_ref,
    w_input_ref,
    out_ref,
):
    here = here_ref[0]

    def fold(n, value):
        source = EXPERTS - 1 - n
        tile = carry_ref[pl.ds(pl.multiple_of(source * 8, 8), 8), :]
        return tile[4:8] + tile[0:4] * value

    entering = lax.fori_loop(0, EXPERTS - 1 - here, fold, jnp.zeros((4, 128), F32))
    for h in range(4):
        cols = slice(h * 128, (h + 1) * 128)
        grad = local_ref[:, cols] + prod_ref[:, cols] * entering[h : h + 1, :]
        d_reset = (grad * kr_ref[:, cols]).astype(BF16)
        d_input = (grad * ki_ref[:, cols]).astype(BF16)
        out_ref[:, cols] = (
            grad * kd_ref[:, cols]
            + dot_bt(d_reset, w_reset_ref[h])
            + dot_bt(d_input, w_input_ref[h])
        ).astype(BF16)


def gathered(a, b):
    left_a, right_b = (shift(a, "tp", 1), shift(b, "tp", -1))
    left_b, right_a = (shift(b, "tp", 1), shift(a, "tp", -1))
    far_a, far_b = (shift(left_a, "tp", 1), shift(right_b, "tp", -1))
    return (a, b, left_a, left_b, right_a, right_b, far_a, far_b)


def collected(value):
    return (value, shift(value, "tp", 1), shift(value, "tp", -1), shift(value, "tp", 2))


def after(value, *others):
    return lax.optimization_barrier((value, others))[0]


def body(
    conv_out,
    gate_in,
    block_states,
    decay_param,
    decay_shift,
    w_reset,
    w_input,
    w_out,
    mixed,
    d_out,
    expert_ids,
    route_weights,
    w_gate,
    w_up,
    w_down,
):
    me = lax.axis_index("tp").astype(jnp.int32).reshape(1)
    here = lax.axis_index(SP).astype(jnp.int32).reshape(1)
    unit = 2 * ROWS * 2048 * HID
    send = local(
        route_kernel,
        "route",
        shape((EXPERTS * BLOCK, WIDTH), BF16),
        1.3e9,
        expert_ids.T,
        route_weights.T,
        mixed,
        d_out,
    )
    slots = local(
        slots_kernel, "slots", shape((TOK, 2), jnp.int32), 1e7, after(expert_ids, send)
    )
    got = exchange(send, SP)
    f_like = shape((TOK, WIDTH), F32)
    slow_rate = jax.nn.softplus(-decay_param)
    merged, act, slope, decay, kr, ki, kd = local(
        forward_kernel,
        "forward",
        (shape((8, TOK, WIDTH), BF16),) + (f_like,) * 6,
        6e9,
        after(conv_out, send),
        gate_in,
        block_states,
        slow_rate.reshape(1, -1),
        decay_shift.reshape(-1, 1),
        w_reset,
        w_input,
        scratch=(pltpu.VMEM((TOK, WIDTH), F32),) * 2,
    )
    got = after(got, merged, slots)
    piece = shape((HALF, WIDTH), BF16)
    full = shape((ROWS, WIDTH), BF16)
    rows_a, rows_b = local(
        sort_kernel, "sort", (Near(full), Near(full)), 1e9, Near(got), sort_matrix()
    )
    pieces = gathered(rows_a, rows_b)
    gate2, up2, down2 = (w_gate[0], w_up[0], w_down[0])
    hid = shape((ROWS, HID), BF16)
    hid_f = shape((ROWS, HID), F32)
    near = local(
        expert_near_kernel,
        "expert_near",
        (hid_f,) * 3,
        2 * unit,
        me,
        *map(Near, pieces[:6]),
        gate2,
        up2,
        down2,
        smem=1,
    )
    merged_x = exchange(after(merged, pieces[3]), XC)
    hidden, d_up, d_linear, far_a, far_b, left, right, own = local(
        expert_far_kernel,
        "expert_far",
        (hid, hid, hid, *map(Near, (piece, piece, full, full)), full),
        3 * unit,
        me,
        *map(Near, pieces[6:]),
        gate2,
        up2,
        down2,
        *near,
        smem=1,
    )
    over_a, over_b = (shift(far_a, "tp", 1), shift(far_b, "tp", -1))
    right_b, left_a = (shift(right[HALF:], "tp", 1), shift(left[:HALF], "tp", -1))
    add = lambda u, v: (u.astype(F32) + v.astype(F32)).astype(BF16)
    right_a = shift(add(right[:HALF], over_a), "tp", 1)
    left_b = shift(add(left[HALF:], over_b), "tp", -1)
    returned = local(
        spread_kernel,
        "spread",
        shape((EXPERTS * BLOCK, WIDTH // 2), BF16),
        1e9,
        after(own, merged_x),
        Near(right_a),
        Near(right_b),
        Near(left_a),
        Near(left_b),
        spread_matrix(),
    )
    back = exchange(returned, SP)
    grads = local(
        expert_grad_kernel,
        "expert_grad",
        (shape((1, 2048, HID), F32), shape((1, 2048, HID), F32), shape((1, HID, 2048), F32)),
        3 * unit,
        me,
        *pieces,
        after(d_up, returned),
        d_linear,
        hidden,
        smem=1,
    )
    back = after(back, grads)
    d_columns, crossing = local(
        combine_kernel,
        "combine",
        (Near(shape((TOK, WIDTH), BF16)), Near(shape((8, TOK // 2, 128), BF16))),
        1e9,
        Near(back),
        slots,
        d_out,
    )
    crossed = exchange(crossing, XC)
    pieces = collected(d_columns)
    columns = collected(crossed)
    grad_gate, local_grad, products, carries = local(
        reverse_kernel,
        "reverse",
        (shape((TOK, WIDTH), BF16), Near(f_like), Near(f_like), shape((EXPERTS * 8, 128), F32)),
        4e9,
        me,
        *map(Near, (after(pieces[0], crossed), *pieces[1:])),
        w_out,
        act,
        slope,
        decay,
        scratch=(pltpu.VMEM((TOK, WIDTH), F32),),
        smem=1,
    )
    carried = exchange(carries, SP)
    grad_part = local(
        project_kernel,
        "project",
        shape((256, WIDTH), BF16),
        1e9,
        me,
        *map(Near, columns),
        Near(merged_x),
        smem=1,
    )
    parts = exchange(grad_part, "z")
    grad_out_proj_t = jnp.sum(parts.reshape(8, -1, WIDTH).astype(F32), axis=0)
    out = local(
        final_kernel,
        "final",
        shape((TOK, WIDTH), BF16),
        2e9,
        here,
        Near(carried),
        Near(local_grad),
        Near(products),
        kr,
        ki,
        kd,
        w_reset,
        w_input,
        smem=1,
    )
    return (*grads, grad_out_proj_t, out, grad_gate)


def solution(mesh):
    torus = Mesh(mesh.devices.reshape(8, 4, 2, mesh.shape["tp"]), ("z", "x", "c", "tp"))
    in_specs = (
        P(SP, "tp"),
        P(SP, "tp"),
        P(SP, "tp"),
        P("tp"),
        P(SP),
        P("tp", None, None),
        P("tp", None, None),
        P("tp", None),
        P(SP, "tp"),
        P(SP, "tp"),
        P(SP, None),
        P(SP, None),
        P(SP, None, "tp"),
        P(SP, None, "tp"),
        P(SP, "tp", None),
    )
    out_specs = (
        P(SP, None, "tp"),
        P(SP, None, "tp"),
        P(SP, "tp", None),
        P(SP, "tp"),
        P(SP, "tp"),
        P(SP, "tp"),
    )
    return jax.shard_map(body, mesh=torus, in_specs=in_specs, out_specs=out_specs, check_vma=False)
```

```python
import jax
import jax.numpy as jnp
import numpy as np
from jax import lax
from jax.experimental import pallas as pl
from jax.experimental.pallas import tpu as pltpu
from jax.sharding import Mesh
from jax.sharding import PartitionSpec as P

SP = ("z", "x", "c")
XC = ("x", "c")
F32 = jnp.float32
BF16 = jnp.bfloat16
VMEM = pl.BlockSpec(memory_space=pltpu.VMEM)
SMEM = pl.BlockSpec(memory_space=pltpu.SMEM)

TOK = 192
WIDTH = 512
EXPERTS = 64
CAP = 12
BLOCK = 2 * CAP
ROWS = EXPERTS * CAP
HALF = ROWS // 2
GROUP = 8 * BLOCK
GROUPS = EXPERTS * BLOCK // GROUP
HID = 256


def dot(a, b):
    return lax.dot_general(a, b, (((1,), (0,)), ((), ())), preferred_element_type=F32)


def dot_bt(a, b):
    return lax.dot_general(a, b, (((1,), (1,)), ((), ())), preferred_element_type=F32)


def dot_at(a, b):
    return lax.dot_general(a, b, (((0,), (0,)), ((), ())), preferred_element_type=F32)


def shape(dims, dtype):
    return jax.ShapeDtypeStruct(dims, dtype)


class Near:
    def __init__(self, value):
        self.value = value


def size(a):
    return a.size * a.dtype.itemsize


def local(kernel, name, outs, flops, *args, scratch=(), smem=0):
    def unwrapped(a):
        return a.value if isinstance(a, Near) else a

    def operand(n, a):
        if isinstance(a, Near):
            return pltpu.with_memory_space_constraint(a.value, pltpu.VMEM)
        if n < smem or a.ndim < 2:
            return a
        return pltpu.with_memory_space_constraint(a, pltpu.HBM)

    def result(o):
        if isinstance(o, Near):
            return pltpu.VMEM(o.value.shape, o.value.dtype)
        return pltpu.HBM(o.shape, o.dtype)

    single = not isinstance(outs, tuple)
    every = (*args, *((outs,) if single else outs))
    staged = sum(size(a) for a in every if not isinstance(a, Near))
    moved = sum(size(unwrapped(a)) for a in every)
    got = pl.pallas_call(
        kernel,
        name=name,
        out_shape=result(outs) if single else tuple(result(o) for o in outs),
        in_specs=[SMEM] * smem + [VMEM] * (len(args) - smem),
        out_specs=VMEM if single else (VMEM,) * len(outs),
        scratch_shapes=list(scratch),
        compiler_params=pltpu.CompilerParams(vmem_limit_bytes=staged + (10 << 20)),
        cost_estimate=pl.CostEstimate(flops=int(flops), bytes_accessed=moved, transcendentals=0),
    )(*[operand(n, a) for n, a in enumerate(args)])
    return got


def shift(value, axis, by):
    n = lax.axis_size(axis)
    return lax.ppermute(value, axis, [(i, (i + by) % n) for i in range(n)])


def exchange(value, axes):
    return lax.all_to_all(value, axes, 0, 0, tiled=True)


def one_hot(mask):
    return jnp.where(mask, 1.0, 0.0).astype(BF16)


def slots_kernel(ids_ref, slots_ref):
    i32 = jnp.int32
    later = one_hot(
        lax.broadcasted_iota(i32, (TOK, TOK), 1) < lax.broadcasted_iota(i32, (TOK, TOK), 0)
    )
    expert_c = lax.broadcasted_iota(i32, (TOK, EXPERTS), 1)
    cols = [ids_ref[:, k : k + 1] for k in range(2)]
    named_c = [c == expert_c for c in cols]
    count_c = dot(later, one_hot(named_c[0] | named_c[1]))
    for k in range(2):
        rank = jnp.sum(jnp.where(named_c[k], count_c, 0.0), axis=1, keepdims=True)
        slots_ref[:, k : k + 1] = cols[k] * BLOCK + rank.astype(i32)


def route_kernel(ids_t_ref, weights_t_ref, mixed_ref, d_out_ref, send_ref):
    i32 = jnp.int32
    before = one_hot(
        lax.broadcasted_iota(i32, (TOK, TOK), 0) < lax.broadcasted_iota(i32, (TOK, TOK), 1)
    )
    expert = lax.broadcasted_iota(i32, (EXPERTS, TOK), 0)
    rows = [ids_t_ref[k : k + 1, :] for k in range(2)]
    named = [r == expert for r in rows]
    count = dot(one_hot(named[0] | named[1]), before)
    slot = [
        rows[k] * BLOCK
        + jnp.sum(jnp.where(named[k], count, 0.0), axis=0, keepdims=True).astype(i32)
        for k in range(2)
    ]
    weights = [weights_t_ref[k : k + 1, :] for k in range(2)]
    mixed = mixed_ref[...]
    d_out = d_out_ref[...]

    def pack(g):
        at = lax.broadcasted_iota(i32, (GROUP, TOK), 0) + g * GROUP
        to_mix = one_hot((slot[0] == at) | (slot[1] == at))
        first, second = (slot[0] + CAP == at, slot[1] + CAP == at)
        to_cot = one_hot(first | second)
        scale = jnp.sum(
            jnp.where(first, weights[0], 0.0) + jnp.where(second, weights[1], 0.0),
            axis=1,
            keepdims=True,
        )
        value = dot(to_mix, mixed) + dot(to_cot, d_out) * scale
        send_ref[pl.ds(pl.multiple_of(g * GROUP, GROUP), GROUP), :] = value.astype(BF16)

    def two(n, carry):
        pack(2 * n)
        pack(2 * n + 1)
        return carry

    lax.fori_loop(0, GROUPS // 2, two, 0)


def sort_matrix():
    matrix = np.zeros((GROUP, GROUP), np.float32)
    for j in range(8):
        for r in range(CAP):
            matrix[j * CAP + r, j * BLOCK + r] = 1
            matrix[GROUP // 2 + j * CAP + r, j * BLOCK + CAP + r] = 1
    return jnp.asarray(matrix, BF16)


def spread_matrix():
    matrix = np.zeros((GROUP, GROUP // 2), np.float32)
    for j in range(8):
        for r in range(BLOCK):
            matrix[j * BLOCK + r, j * CAP + r % CAP] = 1
    return jnp.asarray(matrix, BF16)


def sort_kernel(got_ref, order_ref, rows_a, rows_b):
    order = order_ref[...]
    half = GROUP // 2
    for g in range(GROUPS):
        out = dot(order, got_ref[g * GROUP : (g + 1) * GROUP, :]).astype(BF16)
        at = (g % (GROUPS // 2)) * half
        rows = rows_a if g < GROUPS // 2 else rows_b
        rows[at : at + half, :] = out[:half]
        rows[HALF + at : HALF + at + half, :] = out[half:]


def block_of(me_ref, step):
    return pl.multiple_of(((me_ref[0] + step) % 4) * WIDTH, WIDTH)


STEPS = (0, 3, 1, 2)


def hidden_terms(me_ref, refs, turns, gate_ref, up_ref, down_ref, h):
    sums = None
    for p, turn in enumerate(turns):
        piece = refs[2 * p + h]
        at = block_of(me_ref, turn)
        mix = piece[:HALF, :]
        terms = (
            dot(mix, gate_ref[pl.ds(at, WIDTH), :]),
            dot(mix, up_ref[pl.ds(at, WIDTH), :]),
            dot_bt(piece[HALF:, :], down_ref[:, pl.ds(at, WIDTH)]),
        )
        sums = terms if sums is None else tuple(a + b for a, b in zip(sums, terms))
    return sums


def expert_near_kernel(me_ref, *refs):
    gate_ref, up_ref, down_ref = refs[6:9]
    for h in range(2):
        rows = slice(h * HALF, (h + 1) * HALF)
        terms = hidden_terms(me_ref, refs[:6], STEPS[:3], gate_ref, up_ref, down_ref, h)
        for term, out in zip(terms, refs[9:]):
            out[rows, :] = term


def expert_far_kernel(me_ref, *refs):
    gate_ref, up_ref, down_ref = refs[2:5]
    near_refs = refs[5:8]
    hidden_ref, d_up_ref, d_linear_ref = refs[8:11]
    far_a, far_b, left_a, left_b, right_a, right_b, own_ref = refs[11:]
    for h in range(2):
        rows = slice(h * HALF, (h + 1) * HALF)
        terms = hidden_terms(me_ref, refs[:2], STEPS[3:], gate_ref, up_ref, down_ref, h)
        up_pre, linear, d_hidden = (a[rows, :] + b for a, b in zip(near_refs, terms))
        sigmoid = jax.nn.sigmoid(up_pre)
        silu = up_pre * sigmoid
        hidden_ref[rows, :] = (silu * linear).astype(BF16)
        d_linear_ref[rows, :] = (d_hidden * silu).astype(BF16)
        slope = linear * sigmoid * (1.0 + up_pre * (1.0 - sigmoid))
        d_up_ref[rows, :] = (d_hidden * slope).astype(BF16)

    def part(rows, turn):
        at = block_of(me_ref, turn)
        return (
            dot_bt(d_up_ref[rows, :], gate_ref[pl.ds(at, WIDTH), :])
            + dot_bt(d_linear_ref[rows, :], up_ref[pl.ds(at, WIDTH), :])
        ).astype(BF16)

    top, low = (slice(0, HALF), slice(HALF, ROWS))
    halves = ((top, far_a, left_a, right_a), (low, far_b, left_b, right_b))
    for rows, far, left, right in halves:
        far[...] = part(rows, 2)
        left[...] = part(rows, 3)
        right[...] = part(rows, 1)
        own_ref[rows, :] = part(rows, 0)


def expert_grad_kernel(me_ref, *refs):
    pieces = refs[:8]
    d_up_ref, d_linear_ref, hidden_ref = refs[8:11]
    grad_gate_ref, grad_up_ref, grad_down_ref = refs[11:]
    top, low = (slice(0, HALF), slice(HALF, ROWS))
    for p in range(4):

        def step(n, carry, halves=(pieces[2 * p], pieces[2 * p + 1]), p=p):
            cols = pl.ds(pl.multiple_of(n * 128, 128), 128)
            at = pl.ds(pl.multiple_of(block_of(me_ref, STEPS[p]) + n * 128, 128), 128)
            mix_a, mix_b = (half[:HALF, cols] for half in halves)
            cot_a, cot_b = (half[HALF:, cols] for half in halves)
            grad_gate_ref[0, at, :] = dot_at(mix_a, d_up_ref[top, :]) + dot_at(
                mix_b, d_up_ref[low, :]
            )
            grad_up_ref[0, at, :] = dot_at(mix_a, d_linear_ref[top, :]) + dot_at(
                mix_b, d_linear_ref[low, :]
            )
            grad_down_ref[0, :, at] = dot_at(hidden_ref[top, :], cot_a) + dot_at(
                hidden_ref[low, :], cot_b
            )
            return carry

        lax.fori_loop(0, 4, step, 0)


def spread_kernel(own_ref, la_ref, lb_ref, ra_ref, rb_ref, order_ref, out_ref):
    order = order_ref[...]
    half = GROUP // 2
    first = (lax.broadcasted_iota(jnp.int32, (GROUP, 1), 0) % BLOCK) < CAP
    for g in range(GROUPS):
        at = (g % (GROUPS // 2)) * half
        from_left, from_right = (la_ref, ra_ref) if g < GROUPS // 2 else (lb_ref, rb_ref)
        total = (
            own_ref[g * half : (g + 1) * half, :].astype(F32)
            + from_left[at : at + half, :].astype(F32)
            + from_right[at : at + half, :].astype(F32)
        ).astype(BF16)
        wide = dot(order, total)
        out_ref[g * GROUP : (g + 1) * GROUP, :] = jnp.where(
            first, wide[:, : WIDTH // 2], wide[:, WIDTH // 2 :]
        ).astype(BF16)


def combine_kernel(back_ref, slots_ref, d_out_ref, out_ref, send_ref):
    at = lax.broadcasted_iota(jnp.int32, (TOK, EXPERTS * BLOCK), 1)
    one, two = (slots_ref[:, 0:1], slots_ref[:, 1:2])
    back = back_ref[...]
    for h in range(2):
        pick = one_hot((one + h * CAP == at) | (two + h * CAP == at))
        cols = slice(h * WIDTH // 2, (h + 1) * WIDTH // 2)
        out_ref[:, cols] = (d_out_ref[:, cols].astype(F32) + dot(pick, back)).astype(BF16)
    source = lax.broadcasted_iota(jnp.int32, (WIDTH, WIDTH), 0)
    target = lax.broadcasted_iota(jnp.int32, (WIDTH, WIDTH), 1)
    wanted = ((target >> 5) & 1) * 256 + (target >> 6) * 32 + (target & 31)
    moved = dot(out_ref[...], one_hot(source == wanted))
    lane = lax.broadcasted_iota(jnp.int32, (TOK // 2, 128), 1)
    for m in range(4):
        top = moved[: TOK // 2, 128 * m : 128 * (m + 1)]
        low = moved[TOK // 2 :, 128 * m : 128 * (m + 1)]
        send_ref[2 * m] = jnp.where(lane < 64, top, pltpu.roll(low, 64, 1)).astype(BF16)
        send_ref[2 * m + 1] = jnp.where(lane < 64, pltpu.roll(top, 64, 1), low).astype(BF16)


def neg_expm1(y):
    small = 1.0 + y * (1.0 / 7.0)
    for n in (6.0, 5.0, 4.0, 3.0, 2.0):
        small = 1.0 + y * small * (1.0 / n)
    return jnp.where(y > -0.5, -y * small, 1.0 - jnp.exp(y))


CHUNK = 16


def forward_kernel(
    conv_ref,
    gate_ref,
    start_ref,
    slow_ref,
    shift_ref,
    w_reset_ref,
    w_input_ref,
    merged_ref,
    act_ref,
    slope_ref,
    decay_ref,
    kr_ref,
    ki_ref,
    kd_ref,
    pre_r,
    pre_i,
):
    for h in range(4):
        cols = slice(h * 128, (h + 1) * 128)
        pre_r[:, cols] = dot(conv_ref[:, cols], w_reset_ref[h])
        pre_i[:, cols] = dot(conv_ref[:, cols], w_input_ref[h])
    row = lax.broadcasted_iota(jnp.int32, (8, WIDTH), 0)
    slow = -8.0 * slow_ref[...]

    def step(c, state):
        rows = pl.ds(pl.multiple_of(c * CHUNK, CHUNK), CHUNK)
        conv = conv_ref[rows, :].astype(F32)
        reset = jax.nn.sigmoid(pre_r[rows, :])
        gate_in = jax.nn.sigmoid(pre_i[rows, :])
        log_decay = reset * slow + shift_ref[rows, :]
        decay = jnp.exp(log_decay)
        norm = jnp.sqrt(neg_expm1(2.0 * log_decay))
        direct = norm * gate_in
        drive = direct * conv
        states, prevs = [], []
        for s in range(0, CHUNK, 8):
            a, b = (decay[s : s + 8], drive[s : s + 8])
            for d in (1, 2, 4):
                keep = row >= d
                b = jnp.where(keep, b + a * pltpu.roll(b, d, 0), b)
                a = jnp.where(keep, a * pltpu.roll(a, d, 0), a)
            now = a * state + b
            prevs.append(jnp.where(row == 0, state, pltpu.roll(now, 1, 0)))
            states.append(now)
            state = now[7:8, :]
        states = jnp.concatenate(states, axis=0)
        prevs = jnp.concatenate(prevs, axis=0)
        x = gate_ref[rows, :].astype(F32)
        c0 = 0.7978845608028654
        t = jnp.tanh(c0 * (x + 0.044715 * x * x * x))
        act = 0.5 * x * (1.0 + t)
        deriv = 0.5 * (1.0 + t) + 0.5 * x * (1.0 - t * t) * (c0 * (1.0 + 0.134145 * x * x))
        merged = (act * states).astype(BF16)
        for k in range(8):
            merged_ref[k, rows, :] = merged
        act_ref[rows, :] = act
        slope_ref[rows, :] = states * deriv
        decay_ref[rows, :] = decay
        d_log = decay * prevs - gate_in * conv * decay * decay / norm
        kr_ref[rows, :] = d_log * slow * reset * (1.0 - reset)
        ki_ref[rows, :] = drive * (1.0 - gate_in)
        kd_ref[rows, :] = direct
        return state

    lax.fori_loop(0, TOK // CHUNK, step, start_ref[...])


def project_kernel(me_ref, p0, p1, p2, p3, merged_ref, out_ref):
    half = TOK // 2
    top = merged_ref[:, :half, :].reshape(8 * half, WIDTH)
    low = merged_ref[:, half:, :].reshape(8 * half, WIDTH)
    for piece, step in zip((p0, p1, p2, p3), STEPS):
        at = pl.multiple_of(((me_ref[0] + step) % 4) * 64, 64)
        value = piece[...].reshape(8 * half, 128)
        total = dot_at(value, top)[:64] + dot_at(value, low)[64:]
        out_ref[pl.ds(at, 64), :] = total.astype(BF16)


def reverse_kernel(
    me_ref,
    p0,
    p1,
    p2,
    p3,
    w_out_ref,
    act_ref,
    slope_ref,
    decay_ref,
    grad_gate_ref,
    local_ref,
    prod_ref,
    carry_ref,
    merged_ref,
):
    total = None
    for piece, step in zip((p0, p1, p2, p3), STEPS):
        one = dot_bt(piece[...], w_out_ref[:, pl.ds(block_of(me_ref, step), WIDTH)])
        total = one if total is None else total + one
    merged_ref[...] = total
    row = lax.broadcasted_iota(jnp.int32, (8, WIDTH), 0)
    steps = TOK // 16

    def step(n, state):
        grad, prod, after = state
        at = pl.multiple_of((steps - 1 - n) * 16, 16)
        rows16 = pl.ds(at, 16)
        d_merged = merged_ref[rows16, :]
        grad_gate_ref[rows16, :] = (d_merged * slope_ref[rows16, :]).astype(BF16)
        d_states = d_merged * act_ref[rows16, :]
        decays = decay_ref[rows16, :]
        for s in (8, 0):
            decay = decays[s : s + 8]
            a = jnp.where(row == 7, after, pltpu.roll(decay, 7, 0))
            b = d_states[s : s + 8]
            for d in (1, 2, 4):
                keep = row < 8 - d
                b = jnp.where(keep, b + a * pltpu.roll(b, 8 - d, 0), b)
                a = jnp.where(keep, a * pltpu.roll(a, 8 - d, 0), a)
            now = b + a * grad
            products = a * prod
            rows8 = pl.ds(pl.multiple_of(at + s, 8), 8)
            local_ref[rows8, :] = now
            prod_ref[rows8, :] = products
            grad, prod, after = (now[0:1, :], products[0:1, :], decay[0:1, :])
        return (grad, prod, after)

    one = jnp.ones((1, WIDTH), F32)
    grad, prod, first = lax.fori_loop(0, steps, step, (jnp.zeros((1, WIDTH), F32), one, one))
    prod, lead = (prod * first, grad * first)
    rows = [prod[:, k * 128 : (k + 1) * 128] for k in range(4)]
    rows += [lead[:, k * 128 : (k + 1) * 128] for k in range(4)]
    tile = jnp.concatenate(rows, axis=0)
    for k in range(EXPERTS):
        carry_ref[8 * k : 8 * k + 8, :] = tile


def final_kernel(
    here_ref,
    carry_ref,
    local_ref,
    prod_ref,
    kr_ref,
    ki_ref,
    kd_ref,
    w_reset_ref,
    w_input_ref,
    out_ref,
):
    here = here_ref[0]

    def fold(n, value):
        source = EXPERTS - 1 - n
        tile = carry_ref[pl.ds(pl.multiple_of(source * 8, 8), 8), :]
        return tile[4:8] + tile[0:4] * value

    entering = lax.fori_loop(0, EXPERTS - 1 - here, fold, jnp.zeros((4, 128), F32))
    for h in range(4):
        cols = slice(h * 128, (h + 1) * 128)
        grad = local_ref[:, cols] + prod_ref[:, cols] * entering[h : h + 1, :]
        d_reset = (grad * kr_ref[:, cols]).astype(BF16)
        d_input = (grad * ki_ref[:, cols]).astype(BF16)
        out_ref[:, cols] = (
            grad * kd_ref[:, cols]
            + dot_bt(d_reset, w_reset_ref[h])
            + dot_bt(d_input, w_input_ref[h])
        ).astype(BF16)


def gathered(a, b):
    left_a, right_b = (shift(a, "tp", 1), shift(b, "tp", -1))
    left_b, right_a = (shift(b, "tp", 1), shift(a, "tp", -1))
    far_a, far_b = (shift(left_a, "tp", 1), shift(right_b, "tp", -1))
    return (a, b, left_a, left_b, right_a, right_b, far_a, far_b)


def collected(value):
    return (value, shift(value, "tp", 1), shift(value, "tp", -1), shift(value, "tp", 2))


def after(value, *others):
    return lax.optimization_barrier((value, others))[0]


def body(
    conv_out,
    gate_in,
    block_states,
    decay_param,
    decay_shift,
    w_reset,
    w_input,
    w_out,
    mixed,
    d_out,
    expert_ids,
    route_weights,
    w_gate,
    w_up,
    w_down,
):
    me = lax.axis_index("tp").astype(jnp.int32).reshape(1)
    here = lax.axis_index(SP).astype(jnp.int32).reshape(1)
    unit = 2 * ROWS * 2048 * HID
    send = local(
        route_kernel,
        "route",
        shape((EXPERTS * BLOCK, WIDTH), BF16),
        1.3e9,
        expert_ids.T,
        route_weights.T,
        mixed,
        d_out,
    )
    slots = local(
        slots_kernel, "slots", shape((TOK, 2), jnp.int32), 1e7, after(expert_ids, send)
    )
    got = exchange(send, SP)
    f_like = shape((TOK, WIDTH), F32)
    slow_rate = jax.nn.softplus(-decay_param)
    merged, act, slope, decay, kr, ki, kd = local(
        forward_kernel,
        "forward",
        (shape((8, TOK, WIDTH), BF16),) + (f_like,) * 6,
        6e9,
        after(conv_out, send),
        gate_in,
        block_states,
        slow_rate.reshape(1, -1),
        decay_shift.reshape(-1, 1),
        w_reset,
        w_input,
        scratch=(pltpu.VMEM((TOK, WIDTH), F32),) * 2,
    )
    got = after(got, merged, slots)
    piece = shape((HALF, WIDTH), BF16)
    full = shape((ROWS, WIDTH), BF16)
    rows_a, rows_b = local(
        sort_kernel, "sort", (Near(full), Near(full)), 1e9, Near(got), sort_matrix()
    )
    pieces = gathered(rows_a, rows_b)
    gate2, up2, down2 = (w_gate[0], w_up[0], w_down[0])
    hid = shape((ROWS, HID), BF16)
    hid_f = shape((ROWS, HID), F32)
    near = local(
        expert_near_kernel,
        "expert_near",
        (hid_f,) * 3,
        2 * unit,
        me,
        *map(Near, pieces[:6]),
        gate2,
        up2,
        down2,
        smem=1,
    )
    merged_x = exchange(after(merged, pieces[3]), XC)
    hidden, d_up, d_linear, far_a, far_b, left_top, left_low, right_top, right_low, own = local(
        expert_far_kernel,
        "expert_far",
        (hid, hid, hid, *map(Near, (piece,) * 6), full),
        3 * unit,
        me,
        *map(Near, pieces[6:]),
        gate2,
        up2,
        down2,
        *near,
        smem=1,
    )
    over_a, over_b = (shift(far_a, "tp", 1), shift(far_b, "tp", -1))
    right_b, left_a = (shift(right_low, "tp", 1), shift(left_top, "tp", -1))
    add = lambda u, v: (u.astype(F32) + v.astype(F32)).astype(BF16)
    right_a = shift(add(right_top, over_a), "tp", 1)
    left_b = shift(add(left_low, over_b), "tp", -1)
    returned = local(
        spread_kernel,
        "spread",
        shape((EXPERTS * BLOCK, WIDTH // 2), BF16),
        1e9,
        after(own, merged_x),
        Near(right_a),
        Near(right_b),
        Near(left_a),
        Near(left_b),
        spread_matrix(),
    )
    back = exchange(returned, SP)
    grads = local(
        expert_grad_kernel,
        "expert_grad",
        (shape((1, 2048, HID), F32), shape((1, 2048, HID), F32), shape((1, HID, 2048), F32)),
        3 * unit,
        me,
        *pieces,
        after(d_up, returned),
        d_linear,
        hidden,
        smem=1,
    )
    back = after(back, grads)
    d_columns, crossing = local(
        combine_kernel,
        "combine",
        (Near(shape((TOK, WIDTH), BF16)), Near(shape((8, TOK // 2, 128), BF16))),
        1e9,
        Near(back),
        slots,
        d_out,
    )
    crossed = exchange(crossing, XC)
    pieces = collected(d_columns)
    columns = collected(crossed)
    grad_gate, local_grad, products, carries = local(
        reverse_kernel,
        "reverse",
        (shape((TOK, WIDTH), BF16), Near(f_like), Near(f_like), shape((EXPERTS * 8, 128), F32)),
        4e9,
        me,
        *map(Near, (after(pieces[0], crossed), *pieces[1:])),
        w_out,
        act,
        slope,
        decay,
        scratch=(pltpu.VMEM((TOK, WIDTH), F32),),
        smem=1,
    )
    carried = exchange(carries, SP)
    grad_part = local(
        project_kernel,
        "project",
        shape((256, WIDTH), BF16),
        1e9,
        me,
        *map(Near, columns),
        Near(merged_x),
        smem=1,
    )
    parts = exchange(grad_part, "z")
    grad_out_proj_t = jnp.sum(parts.reshape(8, -1, WIDTH).astype(F32), axis=0)
    out = local(
        final_kernel,
        "final",
        shape((TOK, WIDTH), BF16),
        2e9,
        here,
        Near(carried),
        Near(local_grad),
        Near(products),
        kr,
        ki,
        kd,
        w_reset,
        w_input,
        smem=1,
    )
    return (*grads, grad_out_proj_t, out, grad_gate)


def solution(mesh):
    torus = Mesh(mesh.devices.reshape(8, 4, 2, mesh.shape["tp"]), ("z", "x", "c", "tp"))
    in_specs = (
        P(SP, "tp"),
        P(SP, "tp"),
        P(SP, "tp"),
        P("tp"),
        P(SP),
        P("tp", None, None),
        P("tp", None, None),
        P("tp", None),
        P(SP, "tp"),
        P(SP, "tp"),
        P(SP, None),
        P(SP, None),
        P(SP, None, "tp"),
        P(SP, None, "tp"),
        P(SP, "tp", None),
    )
    out_specs = (
        P(SP, None, "tp"),
        P(SP, None, "tp"),
        P(SP, "tp", None),
        P(SP, "tp"),
        P(SP, "tp"),
        P(SP, "tp"),
    )
    return jax.shard_map(body, mesh=torus, in_specs=in_specs, out_specs=out_specs, check_vma=False)
```
